32 devices in a mesh: fs: 8 (over z, y), tp: 4 (over x, core).
Axes of the slice: x: 2, y: 2, z: 4, core: 2. Of those that a mesh axis runs over, the one named last changes fastest.
Arguments:
- tokens: bfloat16 [3072, 2048], P('fs'), may hold values from -6 to 6
- first_norm_scale: float32 [2048], replicated, may hold values from 0.1 to 1.9
- recurrent_branch_matrix: bfloat16 [2048, 1024], P('fs', 'tp'), may hold values from -0.125 to 0.125
- gelu_gate_matrix: bfloat16 [2048, 1024], P('fs', 'tp'), may hold values from -0.125 to 0.125
- filter_taps_weight: bfloat16 [4, 1024], P(None, 'tp'), may hold values from -3 to 3
- recurrence_gate_blocks: bfloat16 [16, 64, 64], P('tp'), may hold values from -0.75 to 0.75
- input_gate_blocks: bfloat16 [16, 64, 64], P('tp'), may hold values from -0.75 to 0.75
- base_decay_logits: float32 [1024], P('tp'), may hold values from 4 to 11
- extra_log_decay: float32 [3072, 1024], P('fs', 'tp'), may hold values from -0.7 to 0
- mixer_output_matrix: bfloat16 [2048, 1024], P('fs', 'tp'), may hold values from -0.5 to 0.5
- second_norm_scale: float32 [2048], replicated, may hold values from 0.1 to 1.9
- mixer_up_matrix: bfloat16 [2048, 4096], P('fs', 'tp'), may hold values from -0.125 to 0.125
- mixer_down_matrix: bfloat16 [2048, 4096], P('fs', 'tp'), may hold values from -0.09375 to 0.09375
Outputs:
- layer_out: bfloat16 [3072, 2048], P(('fs', 'tp'))
The draws below stay inside these ranges and needn't reach their ends.
All inputs are finite; a program needn't handle non-finite values.
Results may differ from the reference program's by a relative error of at most 0.022.
Values may be sent and summed in bfloat16 or wider, within the bound.
A program may use at most 64 MiB of HBM per device.

```python
import jax
import jax.numpy as jnp
from jax import lax

D = 2048
R_BLOCKS = 16
BLOCK_DIM = 64
RECURRENT_WIDTH = 1024
FF = 4096
TAPS = 4
SEQUENCE_LENGTH = 384
TOKENS = 3072
N_FS = 8
N_TP = 4


def draw_base_decay_logits(key, part):
    pick_key, quick_key, slow_key = jax.random.split(jax.random.fold_in(key, 11), 3)
    quick_share = 0.5
    quick_mask = jax.random.uniform(pick_key, (RECURRENT_WIDTH,), jnp.float32) < quick_share
    quick_speed = jnp.exp(jax.random.uniform(quick_key, (RECURRENT_WIDTH,), jnp.float32, jnp.log(0.004), jnp.log(0.012)))
    slow_speed = jnp.exp(jax.random.uniform(slow_key, (RECURRENT_WIDTH,), jnp.float32, jnp.log(0.03), jnp.log(0.25))) / SEQUENCE_LENGTH
    speeds = jnp.where(quick_mask, quick_speed, slow_speed)
    return (-speeds - jnp.log(-jnp.expm1(-speeds))).astype(jnp.float32)


def draw_extra_log_decay(key, part):
    place_key, depth_key = jax.random.split(jax.random.fold_in(key, 23))
    marked = jax.random.uniform(place_key, (TOKENS, 1), jnp.float32) < 4.0 / SEQUENCE_LENGTH
    kept = jax.random.uniform(depth_key, (TOKENS, RECURRENT_WIDTH), jnp.float32, 0.5, 0.8)
    return jnp.where(marked, jnp.log(kept), 0.0).astype(jnp.float32)


def steps_of(key, shape, shards, smallest, top_value):
    factor_of, own = 1.0, jax.random.fold_in(key, 6)
    for dim, parts in shards:
        steps = jnp.exp(jax.random.uniform(jax.random.fold_in(own, dim), (parts,), jnp.float32, smallest / len(shards), top_value / len(shards)))
        factor_of = factor_of * jnp.repeat(steps, shape[dim] // parts).reshape([-1 if axis == dim else 1 for axis in range(len(shape))])
    return factor_of


def noise(rng, dims, spread, most, shards=(), dtype=jnp.bfloat16):
    values = jax.random.normal(rng, dims, jnp.float32) * spread
    if len(shards) > 0:
        values = steps_of(rng, dims, shards, -0.22, 0.18) * values
    return jnp.clip(values, min=-most, max=most).astype(dtype)


def setup_inputs(seed: int = 0) -> dict:
    keys = jax.random.split(jax.random.key(seed), 14)
    tokens = noise(keys[0], (TOKENS, D), 1.0, 6.0, ((0, 8),))
    first_norm_scale = jnp.clip(1.0 + 0.18 * jax.random.normal(keys[1], (D,), jnp.float32), 0.1, 1.9)
    recurrent_branch_matrix = noise(keys[2], (D, RECURRENT_WIDTH), D ** -0.5, 0.125, ((0, 8), (1, 4)))
    gelu_gate_matrix = noise(keys[3], (D, RECURRENT_WIDTH), D ** -0.5, 0.125, ((0, 8), (1, 4)))
    filter_taps_weight = noise(keys[4], (TAPS, RECURRENT_WIDTH), TAPS ** -0.5, 3.0, ((1, 4),))
    recurrence_gate_blocks = noise(keys[5], (R_BLOCKS, BLOCK_DIM, BLOCK_DIM), BLOCK_DIM ** -0.5, 0.75, ((0, 4),))
    input_gate_blocks = noise(keys[6], (R_BLOCKS, BLOCK_DIM, BLOCK_DIM), BLOCK_DIM ** -0.5, 0.75, ((0, 4),))
    base_decay_logits = draw_base_decay_logits(jax.random.fold_in(keys[13], 71), 0)
    extra_log_decay = draw_extra_log_decay(jax.random.fold_in(keys[13], 71), 0)
    mixer_output_matrix = noise(keys[9], (D, RECURRENT_WIDTH), (RECURRENT_WIDTH // 9) ** -0.5, 0.5, ((0, 8), (1, 4)))
    second_norm_scale = jnp.clip(1.0 + 0.18 * jax.random.normal(keys[10], (D,), jnp.float32), 0.1, 1.9)
    mixer_up_matrix = noise(keys[11], (D, FF), D ** -0.5, 0.125, ((0, 8), (1, 4)))
    mixer_down_matrix = noise(keys[12], (D, FF), FF ** -0.5, 0.09375, ((0, 8), (1, 4)))
    return dict(tokens=tokens, first_norm_scale=first_norm_scale, recurrent_branch_matrix=recurrent_branch_matrix, gelu_gate_matrix=gelu_gate_matrix, filter_taps_weight=filter_taps_weight, recurrence_gate_blocks=recurrence_gate_blocks, input_gate_blocks=input_gate_blocks, base_decay_logits=base_decay_logits, extra_log_decay=extra_log_decay, mixer_output_matrix=mixer_output_matrix, second_norm_scale=second_norm_scale, mixer_up_matrix=mixer_up_matrix, mixer_down_matrix=mixer_down_matrix)


epsilon = 1e-06
decay_rate_scale = 8.0

def rms_scaled(sequence_token_rows, scales):
    widened = sequence_token_rows.astype(jnp.float32)
    mean_square = lax.optimization_barrier(jnp.mean(widened * widened, axis=-1, keepdims=True))
    return (widened * lax.rsqrt(mean_square + epsilon) * scales).astype(jnp.bfloat16)

def linear_combine(earlier, later):
    return (earlier[0] * later[0], later[0] * earlier[1] + later[1])

def causal_taps(branch, filter_taps_weight):
    tap_count = filter_taps_weight.shape[0]
    positions = branch.shape[0]
    padded = jnp.pad(branch.astype(jnp.float32), ((tap_count - 1, 0), (0, 0)))
    running = jnp.zeros(branch.shape, jnp.float32)
    for offset in range(tap_count):
        running = running + padded[offset:offset + positions] * filter_taps_weight[offset].astype(jnp.float32)
    return running.astype(jnp.bfloat16)

def block_map(convolved, blocks):
    positions, channels = convolved.shape
    grouped = convolved.astype(jnp.float32).reshape(positions, blocks.shape[0], blocks.shape[1])
    mapped = jnp.einsum('sgi,gij->sgj', grouped, blocks.astype(jnp.float32))
    return jax.nn.sigmoid(mapped.reshape(positions, channels))

def grouped_sum(left, right, groups):
    width_each = left.shape[1] // groups
    running = jnp.zeros((left.shape[0], right.shape[0]), jnp.float32)
    for column_group in range(groups):
        begin_col = column_group * width_each
        partial_value = jnp.dot(left[:, begin_col:begin_col + width_each], right[:, begin_col:begin_col + width_each].T, preferred_element_type=jnp.float32)
        rounded = lax.optimization_barrier(partial_value.astype(jnp.bfloat16))
        running = running + rounded.astype(jnp.float32)
    return running

def reference(tokens, first_norm_scale, recurrent_branch_matrix, gelu_gate_matrix, filter_taps_weight, recurrence_gate_blocks, input_gate_blocks, base_decay_logits, extra_log_decay, mixer_output_matrix, second_norm_scale, mixer_up_matrix, mixer_down_matrix):

    def single_sequence(input_values):
        sequence_token_rows, extra_decays = input_values
        normed = rms_scaled(sequence_token_rows, first_norm_scale)
        branch = jnp.dot(normed, recurrent_branch_matrix, preferred_element_type=jnp.float32).astype(jnp.bfloat16)
        gate_branch = jnp.dot(normed, gelu_gate_matrix, preferred_element_type=jnp.float32).astype(jnp.bfloat16)
        convolved = causal_taps(branch, filter_taps_weight)
        recurrence_gate_value = block_map(convolved, recurrence_gate_blocks)
        admission = block_map(convolved, input_gate_blocks)
        log_keep_factor = decay_rate_scale * recurrence_gate_value * jax.nn.log_sigmoid(base_decay_logits) + extra_decays
        retain = jnp.exp(log_keep_factor)
        driven = jnp.sqrt(-jnp.expm1(2.0 * log_keep_factor)) * (admission * convolved.astype(jnp.float32))
        memory = lax.associative_scan(linear_combine, (retain, driven), axis=0)[1]
        recurrent = (memory * jax.nn.gelu(gate_branch.astype(jnp.float32))).astype(jnp.bfloat16)
        mixer_out = grouped_sum(recurrent, mixer_output_matrix, N_TP)
        residual = (sequence_token_rows.astype(jnp.float32) + mixer_out).astype(jnp.bfloat16)
        normed_mid = rms_scaled(residual, second_norm_scale)
        raised = jnp.dot(normed_mid, mixer_up_matrix, preferred_element_type=jnp.float32)
        hidden = jnp.square(jax.nn.relu(raised)).astype(jnp.bfloat16)
        channel_sum = grouped_sum(hidden, mixer_down_matrix, N_TP)
        return (residual.astype(jnp.float32) + channel_sum).astype(jnp.bfloat16)
    reshaped_values = tokens.reshape(N_FS, SEQUENCE_LENGTH, D)
    extra_decay_reshaped = extra_log_decay.reshape(N_FS, SEQUENCE_LENGTH, RECURRENT_WIDTH)
    output_values = lax.map(single_sequence, (reshaped_values, extra_decay_reshaped))
    return output_values.reshape(N_FS * SEQUENCE_LENGTH, D)
```

```python
import functools

import jax
import jax.numpy as jnp
from jax import lax
from jax.experimental import pallas as pl
from jax.experimental.pallas import tpu as pltpu
from jax.sharding import PartitionSpec as P

epsilon = 1e-06
decay_rate_scale = 8.0


def rms_scaled(sequence_token_rows, scales):
    widened = sequence_token_rows.astype(jnp.float32)
    mean_square = jnp.mean(widened * widened, axis=-1, keepdims=True)
    return (widened * lax.rsqrt(mean_square + epsilon) * scales).astype(jnp.bfloat16)


def linear_combine(earlier, later):
    return (earlier[0] * later[0], later[0] * earlier[1] + later[1])


def causal_taps(branch, filter_taps_weight):
    tap_count = filter_taps_weight.shape[0]
    positions = branch.shape[0]
    padded = jnp.pad(branch.astype(jnp.float32), ((tap_count - 1, 0), (0, 0)))
    running = jnp.zeros(branch.shape, jnp.float32)
    for offset in range(tap_count):
        running = running + padded[offset : offset + positions] * filter_taps_weight[offset].astype(
            jnp.float32
        )
    return running.astype(jnp.bfloat16)


def block_map(convolved, blocks):
    positions, channels = convolved.shape
    grouped = convolved.reshape(positions, blocks.shape[0], blocks.shape[1])
    mapped = jnp.einsum("sgi,gij->sgj", grouped, blocks, preferred_element_type=jnp.float32)
    return jax.nn.sigmoid(mapped.reshape(positions, channels))


def contract_columns(left, right):
    return lax.dot_general(
        left, right, (((1,), (1,)), ((), ())), preferred_element_type=jnp.float32
    )


def local(
    tokens,
    first_norm_scale,
    recurrent_branch_matrix,
    gelu_gate_matrix,
    filter_taps_weight,
    recurrence_gate_blocks,
    input_gate_blocks,
    base_decay_logits,
    extra_log_decay,
    mixer_output_matrix,
    second_norm_scale,
    mixer_up_matrix,
    mixer_down_matrix,
):
    positions = tokens.shape[0]
    own_count = positions // lax.axis_size("tp")
    normed = rms_scaled(tokens, first_norm_scale)
    branch_sum = jnp.dot(
        normed,
        lax.all_gather(recurrent_branch_matrix, "fs", axis=0, tiled=True),
        preferred_element_type=jnp.float32,
    )
    gate_sum = jnp.dot(
        normed,
        lax.all_gather(gelu_gate_matrix, "fs", axis=0, tiled=True),
        preferred_element_type=jnp.float32,
    )
    branch = branch_sum.astype(jnp.bfloat16)
    gate_branch = gate_sum.astype(jnp.bfloat16)
    out_full = lax.all_gather(mixer_output_matrix, "fs", axis=0, tiled=True)
    convolved = causal_taps(branch, filter_taps_weight)
    recurrence_gate_value = block_map(convolved, recurrence_gate_blocks)
    admission = block_map(convolved, input_gate_blocks)
    log_keep_factor = (
        decay_rate_scale * recurrence_gate_value * jax.nn.log_sigmoid(base_decay_logits)
        + extra_log_decay
    )
    retain = jnp.exp(log_keep_factor)
    driven = jnp.sqrt(-jnp.expm1(2.0 * log_keep_factor)) * (
        admission * convolved.astype(jnp.float32)
    )
    memory = lax.associative_scan(linear_combine, (retain, driven), axis=0)[1]
    recurrent = (memory * jax.nn.gelu(gate_branch.astype(jnp.float32))).astype(jnp.bfloat16)
    up_full = lax.all_gather(mixer_up_matrix, "fs", axis=0, tiled=True)
    whole_sum = lax.psum(contract_columns(recurrent, out_full).astype(jnp.bfloat16), "tp").astype(
        jnp.float32
    )
    residual_all = (tokens.astype(jnp.float32) + whole_sum).astype(jnp.bfloat16)
    raised = jnp.dot(
        rms_scaled(residual_all, second_norm_scale), up_full, preferred_element_type=jnp.float32
    )
    hidden = jnp.square(jax.nn.relu(raised)).astype(jnp.bfloat16)
    residual = lax.dynamic_slice_in_dim(
        residual_all, lax.axis_index("tp") * own_count, own_count, 0
    )
    down_full = lax.all_gather(mixer_down_matrix, "fs", axis=0, tiled=True)
    channel_sum = lax.psum_scatter(
        contract_columns(hidden, down_full).astype(jnp.bfloat16),
        "tp",
        scatter_dimension=0,
        tiled=True,
    ).astype(jnp.float32)
    return (residual.astype(jnp.float32) + channel_sum).astype(jnp.bfloat16)


MESH = pl.DeviceIdType.MESH
Y_SIZE = 2
MIX_GROUPS = 4
DOWN_GROUPS = 8


def fits(mesh):
    n_fs, n_tp = mesh.shape["fs"], mesh.shape["tp"]
    return n_tp == 2 * Y_SIZE and n_fs == 4 * Y_SIZE


def shifted_down(values, by, fill):
    if by % 8 == 0:
        top = jnp.full((by, values.shape[1]), fill, values.dtype)
        return jnp.concatenate([top, values[: values.shape[0] - by]], axis=0)
    rows = lax.broadcasted_iota(jnp.int32, values.shape, 0)
    return jnp.where(rows < by, fill, pltpu.roll(values, by, 0))


def one_minus_exp(exponent):
    series = 1.0
    for order in range(8, 1, -1):
        series = 1.0 + exponent * (1.0 / order) * series
    return jnp.where(exponent > -0.35, -exponent * series, 1.0 - jnp.exp(exponent))


def fused(
    nz,
    tok_in, scale1, wb, wg, taps, rblk, iblk, logits, extra_in, wo, scale2, wu, wd,
    out,
    normed, fb, fg, fo, fu, fd, rdiag, idiag, tok, extra,
    part1, pair1, give1, got1, res, mid, hidden,
    part2, pair2, xgive, xgot, zgive, zgot,
    z_send, y_send, w_recv, r_send, r_recv, a_send, a_recv, b_send, b_recv, l_sem,
):
    f = lax.axis_index("fs")
    t = lax.axis_index("tp")
    z, y = f // Y_SIZE, f % Y_SIZE
    x, c = t // 2, t % 2
    last = nz - 1
    parity = z % 2
    zmate = z + 1 - 2 * parity
    ymate = z * Y_SIZE + (1 - y)
    xmate = (1 - x) * 2 + c
    cmate = x * 2 + (1 - c)
    diagonal = (1 - x) * 2 + (1 - c)
    rows, width = tok.shape
    own_rows = out.shape[0]
    depth = wb.shape[0]
    half = depth // 2
    units = fu.shape[1]

    early = [
        pltpu.make_async_copy(tok_in, tok, l_sem.at[0]),
        pltpu.make_async_copy(extra_in, extra, l_sem.at[1]),
    ]
    for copy in early:
        copy.start()
    barrier = pltpu.get_barrier_semaphore()
    for k in range(1, nz):
        other = lax.rem(z + k, nz) * Y_SIZE + y
        pl.semaphore_signal(barrier, inc=1, device_id={"fs": other, "tp": t}, device_id_type=MESH)
    pl.semaphore_signal(barrier, inc=1, device_id={"fs": ymate, "tp": t}, device_id_type=MESH)
    for other in (xmate, cmate):
        pl.semaphore_signal(barrier, inc=1, device_id={"fs": f, "tp": other}, device_id_type=MESH)
    pl.semaphore_wait(barrier, nz + 2)

    sent = []

    def start(pred, copy):
        if pred is None:
            copy.start()
        else:
            pl.when(pred)(copy.start)
        sent.append((pred, copy))

    plain = (wb, wg, wo)
    whole = (fb, fg, fo)

    def source(g, way_parity):
        if g < 3:
            return plain[g]
        w = wu if g < 5 else wd
        first = half * ((g - 3) % 2)
        return w.at[
            pl.ds(first, half), pl.ds(pl.multiple_of(way_parity * units, units), units)
        ]

    def slot(g, zs, ys):
        if g < 3:
            return whole[g].at[pl.ds(pl.multiple_of((zs * Y_SIZE + ys) * depth, depth), depth), :]
        if g < 5:
            at = (zs * Y_SIZE + ys) * depth + (g - 3) * half
            return fu.at[pl.ds(pl.multiple_of(at, half), half), :]
        at = ((zs * 2 + (g - 5)) * Y_SIZE + ys) * half
        return fd.at[pl.ds(pl.multiple_of(at, half), half), :]

    def z_copy(g, src, zs, zt, index):
        return pltpu.make_async_remote_copy(
            src_ref=src,
            dst_ref=slot(g, zs, y),
            send_sem=z_send.at[g, index],
            recv_sem=w_recv.at[g, zs * Y_SIZE + y],
            device_id={"fs": zt * Y_SIZE + y, "tp": t},
            device_id_type=MESH,
        )

    def y_copy(g, src, zs):
        return pltpu.make_async_remote_copy(
            src_ref=src,
            dst_ref=slot(g, zs, y),
            send_sem=y_send.at[g, zs],
            recv_sem=w_recv.at[g, zs * Y_SIZE + y],
            device_id={"fs": ymate, "tp": t},
            device_id_type=MESH,
        )

    def take(g, zs, ys):
        here = slot(g, zs, ys)
        pltpu.make_async_remote_copy(
            src_ref=here,
            dst_ref=here,
            send_sem=y_send.at[g, zs],
            recv_sem=w_recv.at[g, zs * Y_SIZE + ys],
            device_id={"fs": ymate, "tp": t},
            device_id_type=MESH,
        ).wait_recv()

    def spread_z(g):
        for d in range(1, 2 if g < 3 else nz):
            for way in (0, 1):
                zt = z + d if way == 0 else z - d
                exists = zt <= last if way == 0 else zt >= 0
                start(exists, z_copy(g, source(g, lax.rem(zt + nz, 2)), z, zt, (d - 1) * 2 + way))

    def own(g):
        start(None, y_copy(g, source(g, parity), z))

    def forward(g, d):
        for way in (0, 1):
            zs = z - d if way == 0 else z + d
            exists = zs >= 0 if way == 0 else zs <= last
            pl.when(exists)(functools.partial(take, g, zs, y))
            if g < 3 and d < last:
                onward = z < last if way == 0 else z > 0
                zt = z + 1 if way == 0 else z - 1
                start(exists & onward, z_copy(g, slot(g, zs, y), zs, zt, d * 2 + way))
            start(exists, y_copy(g, slot(g, zs, y), zs))

    def take_across(g):
        for zs in range(nz):
            take(g, zs, 1 - y)

    def near_copy(src, dst, device, index, send, recv):
        copy = pltpu.make_async_remote_copy(
            src_ref=src,
            dst_ref=dst,
            send_sem=send.at[index],
            recv_sem=recv.at[index],
            device_id=device,
            device_id_type=MESH,
        )
        copy.start()
        sent.append((None, copy))
        return copy

    to_x = {"fs": f, "tp": xmate}
    to_c = {"fs": f, "tp": cmate}
    to_z = {"fs": zmate * Y_SIZE + y, "tp": t}

    spread_z(0)
    own(0)
    spread_z(1)
    own(1)

    stays = [
        pltpu.make_async_copy(source(g, parity), slot(g, z, y), l_sem.at[2 + g]) for g in range(7)
    ]
    for copy in stays:
        copy.start()
    block = rblk.shape[1]
    for blocks, diag in ((rblk, rdiag), (iblk, idiag)):
        diag[...] = jnp.zeros_like(diag)
        for b in range(rblk.shape[0]):
            diag[b * block : (b + 1) * block, b * block : (b + 1) * block] = blocks[b]

    for copy in early:
        copy.wait()

    def norm_rows(i, carry):
        at = pl.ds(pl.multiple_of(i * 32, 32), 32)
        normed[at, :] = rms_scaled(tok[at, :], scale1[...])
        return carry

    lax.fori_loop(0, rows // 32, norm_rows, 0)

    forward(0, 1)
    forward(1, 1)
    spread_z(2)
    forward(0, 2)
    own(2)
    forward(1, 2)
    forward(0, 3)
    forward(1, 3)
    forward(2, 1)
    forward(2, 2)
    spread_z(3)
    own(3)
    forward(2, 3)
    spread_z(4)
    spread_z(5)
    for copy in stays:
        copy.wait()
    take_across(0)

    branch = jnp.dot(normed[...], fb[...], preferred_element_type=jnp.float32)
    branch = branch.astype(jnp.bfloat16).astype(jnp.float32)
    tap_count = taps.shape[0]
    running = branch * taps[tap_count - 1 : tap_count, :].astype(jnp.float32)
    for offset in range(tap_count - 1):
        by = tap_count - 1 - offset
        running = running + shifted_down(branch, by, 0.0) * taps[offset : offset + 1, :].astype(
            jnp.float32
        )
    convolved = running.astype(jnp.bfloat16)
    rate = jax.nn.sigmoid(jnp.dot(convolved, rdiag[...], preferred_element_type=jnp.float32))
    admission = jax.nn.sigmoid(jnp.dot(convolved, idiag[...], preferred_element_type=jnp.float32))
    base = -jnp.log1p(jnp.exp(-logits[...]))
    log_keep = decay_rate_scale * rate * base + extra[...]
    keep = jnp.exp(log_keep)
    memory = jnp.sqrt(one_minus_exp(2.0 * log_keep)) * (admission * convolved.astype(jnp.float32))
    by = 1
    while by < rows:
        memory = keep * shifted_down(memory, by, 0.0) + memory
        if 2 * by < rows:
            keep = keep * shifted_down(keep, by, 1.0)
        by *= 2
    take_across(1)
    gate = jnp.dot(normed[...], fg[...], preferred_element_type=jnp.float32)
    gate = gate.astype(jnp.bfloat16).astype(jnp.float32)
    recurrent = (memory * jax.nn.gelu(gate)).astype(jnp.bfloat16)

    own(4)
    forward(3, 1)

    side = z // (nz // 2)
    inner = z + side * (last - 2 * z)
    ranks = [inner, 1 - inner] + list(range(2, nz))
    order = [rank + side * (last - 2 * rank) for rank in ranks]
    span = width // MIX_GROUPS
    own_at = pl.ds(pl.multiple_of(t * own_rows, own_rows), own_rows)
    firsts, seconds = [], []

    def mix_columns(j):
        return pl.ds(pl.multiple_of(order[j] * span, span), span)

    def mix_first(j):
        firsts[j].wait_recv()
        away = part1[j, 1 - x, c].astype(jnp.float32) + pair1[j, 1 - x].astype(jnp.float32)
        give1[j] = away.astype(jnp.bfloat16)
        seconds.append(
            near_copy(give1.at[j], got1.at[j], to_x, MIX_GROUPS + j, r_send, r_recv)
        )

    def mix_second(j):
        seconds[j].wait_recv()
        mixed = part1[j, x, c].astype(jnp.float32) + pair1[j, x].astype(jnp.float32)
        mixed = mixed + got1[j].astype(jnp.float32)
        at = mix_columns(j)
        res[:, at] = (tok[own_at, at].astype(jnp.float32) + mixed).astype(jnp.bfloat16)

    for j in range(MIX_GROUPS):
        take(2, order[j], 1 - y)
        product = contract_columns(recurrent, fo[mix_columns(j), :])
        part1[j] = product.astype(jnp.bfloat16).reshape(2, 2, own_rows, span)
        firsts.append(
            near_copy(part1.at[j, :, 1 - c], pair1.at[j], to_c, j, r_send, r_recv)
        )
        if j > 0:
            mix_first(j - 1)
        if j > 1:
            mix_second(j - 2)
    mix_first(MIX_GROUPS - 1)
    forward(4, 1)
    forward(3, 2)
    mix_second(MIX_GROUPS - 2)
    mix_second(MIX_GROUPS - 1)

    mid[parity, t] = rms_scaled(res[...], scale2[...])
    mine = mid.at[parity, t]
    theirs = mid.at[1 - parity, t]
    near_copy(mine, mine, to_x, 1, a_send, a_recv)
    near_copy(mine, mine, to_z, 0, a_send, a_recv)
    near_copy(mine, mine, to_c, 2, a_send, a_recv)
    spread_z(6)

    def arrived(par, who, index):
        here = mid.at[par, who]
        pltpu.make_async_remote_copy(
            src_ref=here,
            dst_ref=here,
            send_sem=a_send.at[index],
            recv_sem=a_recv.at[index],
            device_id=to_c,
            device_id_type=MESH,
        ).wait_recv()
        return here

    forward(4, 2)
    forward(3, 3)
    forward(4, 3)
    own(5)
    arrived(1 - parity, t, 0)
    near_copy(theirs, theirs, to_x, 3, a_send, a_recv)
    near_copy(theirs, theirs, to_c, 4, a_send, a_recv)
    beside = arrived(parity, xmate, 1)
    near_copy(beside, beside, to_c, 5, a_send, a_recv)
    own(6)
    forward(5, 1)
    arrived(parity, cmate, 2)
    arrived(parity, diagonal, 5)
    take_across(3)
    take_across(4)

    tile = 256

    def up(par):
        def up_tile(i, carry):
            at = pl.ds(pl.multiple_of(i * tile, tile), tile)
            raised = jnp.dot(
                mid[par].reshape(rows, width), fu[:, at], preferred_element_type=jnp.float32
            )
            hidden[par, :, at] = jnp.square(jnp.maximum(raised, 0.0)).astype(jnp.bfloat16)
            return carry

        lax.fori_loop(0, units // tile, up_tile, 0)

    up(parity)
    forward(6, 1)
    forward(5, 2)
    beside = arrived(1 - parity, xmate, 3)
    near_copy(beside, beside, to_c, 6, a_send, a_recv)
    arrived(1 - parity, cmate, 4)
    arrived(1 - parity, diagonal, 6)
    up(1 - parity)

    narrow = width // DOWN_GROUPS
    exchanges = [[], [], []]

    def place(j):
        return j // 2 + side * (last - 2 * (j // 2))

    def down_first(j):
        exchanges[0][j].wait_recv()
        for par in range(2):
            away = part2[j, par, 1 - x, c].astype(jnp.float32)
            away = away + pair2[j, par, 1 - x].astype(jnp.float32)
            xgive[j, par] = away.astype(jnp.bfloat16)
        exchanges[1].append(
            near_copy(xgive.at[j], xgot.at[j], to_x, DOWN_GROUPS + j, b_send, b_recv)
        )

    def partial_sum(j, par):
        total = part2[j, par, x, c].astype(jnp.float32) + pair2[j, par, x].astype(jnp.float32)
        return total + xgot[j, par].astype(jnp.float32)

    def down_second(j):
        exchanges[1][j].wait_recv()
        zgive[j] = partial_sum(j, 1 - parity).astype(jnp.bfloat16)
        exchanges[2].append(
            near_copy(zgive.at[j], zgot.at[j], to_z, 2 * DOWN_GROUPS + j, b_send, b_recv)
        )

    def down_third(j):
        exchanges[2][j].wait_recv()
        total = partial_sum(j, parity) + zgot[j].astype(jnp.float32)
        for ys in range(Y_SIZE):
            first = (place(j) * Y_SIZE + ys) * depth + (j % 2) * half
            at = pl.ds(pl.multiple_of(first, half), half)
            out[:, at] = (
                res[:, at].astype(jnp.float32) + total[:, ys * half : (ys + 1) * half]
            ).astype(jnp.bfloat16)

    ahead = {0: [(6, 2), (5, 3)], 1: [(6, 3)]}
    for j in range(DOWN_GROUPS):
        for g, d in ahead.get(j, []):
            forward(g, d)
        q = place(j)
        take(5 + j % 2, q, 1 - y)
        at = pl.ds(pl.multiple_of((q * 2 + j % 2) * narrow, narrow), narrow)
        product = contract_columns(hidden[...].reshape(2 * rows, units), fd[at, :])
        part2[j] = product.astype(jnp.bfloat16).reshape(2, 2, 2, own_rows, narrow)
        exchanges[0].append(
            near_copy(part2.at[j, :, :, 1 - c], pair2.at[j], to_c, j, b_send, b_recv)
        )
        if j > 0:
            down_first(j - 1)
        if j > 1:
            down_second(j - 2)
        if j > 2:
            down_third(j - 3)
    down_first(DOWN_GROUPS - 1)
    down_second(DOWN_GROUPS - 2)
    down_third(DOWN_GROUPS - 3)
    down_second(DOWN_GROUPS - 1)
    down_third(DOWN_GROUPS - 2)
    down_third(DOWN_GROUPS - 1)

    for pred, copy in sent:
        if pred is None:
            copy.wait_send()
        else:
            pl.when(pred)(copy.wait_send)


def fused_local(
    mesh,
    tokens,
    first_norm_scale,
    recurrent_branch_matrix,
    gelu_gate_matrix,
    filter_taps_weight,
    recurrence_gate_blocks,
    input_gate_blocks,
    base_decay_logits,
    extra_log_decay,
    mixer_output_matrix,
    second_norm_scale,
    mixer_up_matrix,
    mixer_down_matrix,
):
    n_fs, n_tp = mesh.shape["fs"], mesh.shape["tp"]
    rows, width = tokens.shape
    own_rows = rows // n_tp
    channels = recurrent_branch_matrix.shape[1]
    units = mixer_up_matrix.shape[1] // 2
    span = width // MIX_GROUPS
    narrow = width // DOWN_GROUPS
    low, high = jnp.bfloat16, jnp.float32
    vmem = pl.BlockSpec(memory_space=pltpu.VMEM)
    hbm = pl.BlockSpec(memory_space=pl.ANY)
    return pl.pallas_call(
        functools.partial(fused, n_fs // Y_SIZE),
        out_shape=jax.ShapeDtypeStruct((own_rows, width), low),
        in_specs=[hbm, vmem, hbm, hbm] + [vmem] * 4 + [hbm, hbm, vmem, hbm, hbm],
        out_specs=vmem,
        scratch_shapes=[
            pltpu.VMEM((rows, width), low),
            pltpu.VMEM((width, channels), low),
            pltpu.VMEM((width, channels), low),
            pltpu.VMEM((width, channels), low),
            pltpu.VMEM((width, units), low),
            pltpu.VMEM((width, units), low),
            pltpu.VMEM((channels, channels), low),
            pltpu.VMEM((channels, channels), low),
            pltpu.VMEM((rows, width), low),
            pltpu.VMEM((rows, channels), high),
            pltpu.VMEM((MIX_GROUPS, 2, 2, own_rows, span), low),
            pltpu.VMEM((MIX_GROUPS, 2, own_rows, span), low),
            pltpu.VMEM((MIX_GROUPS, own_rows, span), low),
            pltpu.VMEM((MIX_GROUPS, own_rows, span), low),
            pltpu.VMEM((own_rows, width), low),
            pltpu.VMEM((2, n_tp, own_rows, width), low),
            pltpu.VMEM((2, rows, units), low),
            pltpu.VMEM((DOWN_GROUPS, 2, 2, 2, own_rows, narrow), low),
            pltpu.VMEM((DOWN_GROUPS, 2, 2, own_rows, narrow), low),
            pltpu.VMEM((DOWN_GROUPS, 2, own_rows, narrow), low),
            pltpu.VMEM((DOWN_GROUPS, 2, own_rows, narrow), low),
            pltpu.VMEM((DOWN_GROUPS, own_rows, narrow), low),
            pltpu.VMEM((DOWN_GROUPS, own_rows, narrow), low),
            pltpu.SemaphoreType.DMA((7, 6)),
            pltpu.SemaphoreType.DMA((7, n_fs // Y_SIZE)),
            pltpu.SemaphoreType.DMA((7, n_fs)),
            pltpu.SemaphoreType.DMA((2 * MIX_GROUPS,)),
            pltpu.SemaphoreType.DMA((2 * MIX_GROUPS,)),
            pltpu.SemaphoreType.DMA((7,)),
            pltpu.SemaphoreType.DMA((7,)),
            pltpu.SemaphoreType.DMA((3 * DOWN_GROUPS,)),
            pltpu.SemaphoreType.DMA((3 * DOWN_GROUPS,)),
            pltpu.SemaphoreType.DMA((9,)),
        ],
        compiler_params=pltpu.CompilerParams(
            collective_id=0, has_side_effects=True, vmem_limit_bytes=60 * 1024 * 1024
        ),
        name="fused_layer",
    )(
        tokens,
        first_norm_scale.reshape(1, width),
        recurrent_branch_matrix,
        gelu_gate_matrix,
        filter_taps_weight,
        recurrence_gate_blocks,
        input_gate_blocks,
        base_decay_logits.reshape(1, channels),
        extra_log_decay,
        mixer_output_matrix,
        second_norm_scale.reshape(1, width),
        mixer_up_matrix,
        mixer_down_matrix,
    )


def solution(mesh):
    in_specs = (
        P("fs", None),
        P(),
        P("fs", "tp"),
        P("fs", "tp"),
        P(None, "tp"),
        P("tp", None, None),
        P("tp", None, None),
        P("tp"),
        P("fs", "tp"),
        P("fs", "tp"),
        P(),
        P("fs", "tp"),
        P("fs", "tp"),
    )
    out_specs = P(("fs", "tp"), None)
    body = functools.partial(fused_local, mesh) if fits(mesh) else local
    return jax.shard_map(body, mesh=mesh, in_specs=in_specs, out_specs=out_specs, check_vma=False)
```

```python
import functools

import jax
import jax.numpy as jnp
from jax import lax
from jax.experimental import pallas as pl
from jax.experimental.pallas import tpu as pltpu
from jax.sharding import PartitionSpec as P

epsilon = 1e-06
decay_rate_scale = 8.0


def rms_scaled(sequence_token_rows, scales):
    widened = sequence_token_rows.astype(jnp.float32)
    mean_square = jnp.mean(widened * widened, axis=-1, keepdims=True)
    return (widened * lax.rsqrt(mean_square + epsilon) * scales).astype(jnp.bfloat16)


def linear_combine(earlier, later):
    return (earlier[0] * later[0], later[0] * earlier[1] + later[1])


def causal_taps(branch, filter_taps_weight):
    tap_count = filter_taps_weight.shape[0]
    positions = branch.shape[0]
    padded = jnp.pad(branch.astype(jnp.float32), ((tap_count - 1, 0), (0, 0)))
    running = jnp.zeros(branch.shape, jnp.float32)
    for offset in range(tap_count):
        running = running + padded[offset : offset + positions] * filter_taps_weight[offset].astype(
            jnp.float32
        )
    return running.astype(jnp.bfloat16)


def block_map(convolved, blocks):
    positions, channels = convolved.shape
    grouped = convolved.reshape(positions, blocks.shape[0], blocks.shape[1])
    mapped = jnp.einsum("sgi,gij->sgj", grouped, blocks, preferred_element_type=jnp.float32)
    return jax.nn.sigmoid(mapped.reshape(positions, channels))


def contract_columns(left, right):
    return lax.dot_general(
        left, right, (((1,), (1,)), ((), ())), preferred_element_type=jnp.float32
    )


def local(
    tokens,
    first_norm_scale,
    recurrent_branch_matrix,
    gelu_gate_matrix,
    filter_taps_weight,
    recurrence_gate_blocks,
    input_gate_blocks,
    base_decay_logits,
    extra_log_decay,
    mixer_output_matrix,
    second_norm_scale,
    mixer_up_matrix,
    mixer_down_matrix,
):
    positions = tokens.shape[0]
    own_count = positions // lax.axis_size("tp")
    normed = rms_scaled(tokens, first_norm_scale)
    branch_sum = jnp.dot(
        normed,
        lax.all_gather(recurrent_branch_matrix, "fs", axis=0, tiled=True),
        preferred_element_type=jnp.float32,
    )
    gate_sum = jnp.dot(
        normed,
        lax.all_gather(gelu_gate_matrix, "fs", axis=0, tiled=True),
        preferred_element_type=jnp.float32,
    )
    branch = branch_sum.astype(jnp.bfloat16)
    gate_branch = gate_sum.astype(jnp.bfloat16)
    out_full = lax.all_gather(mixer_output_matrix, "fs", axis=0, tiled=True)
    convolved = causal_taps(branch, filter_taps_weight)
    recurrence_gate_value = block_map(convolved, recurrence_gate_blocks)
    admission = block_map(convolved, input_gate_blocks)
    log_keep_factor = (
        decay_rate_scale * recurrence_gate_value * jax.nn.log_sigmoid(base_decay_logits)
        + extra_log_decay
    )
    retain = jnp.exp(log_keep_factor)
    driven = jnp.sqrt(-jnp.expm1(2.0 * log_keep_factor)) * (
        admission * convolved.astype(jnp.float32)
    )
    memory = lax.associative_scan(linear_combine, (retain, driven), axis=0)[1]
    recurrent = (memory * jax.nn.gelu(gate_branch.astype(jnp.float32))).astype(jnp.bfloat16)
    up_full = lax.all_gather(mixer_up_matrix, "fs", axis=0, tiled=True)
    whole_sum = lax.psum(contract_columns(recurrent, out_full).astype(jnp.bfloat16), "tp").astype(
        jnp.float32
    )
    residual_all = (tokens.astype(jnp.float32) + whole_sum).astype(jnp.bfloat16)
    raised = jnp.dot(
        rms_scaled(residual_all, second_norm_scale), up_full, preferred_element_type=jnp.float32
    )
    hidden = jnp.square(jax.nn.relu(raised)).astype(jnp.bfloat16)
    residual = lax.dynamic_slice_in_dim(
        residual_all, lax.axis_index("tp") * own_count, own_count, 0
    )
    down_full = lax.all_gather(mixer_down_matrix, "fs", axis=0, tiled=True)
    channel_sum = lax.psum_scatter(
        contract_columns(hidden, down_full).astype(jnp.bfloat16),
        "tp",
        scatter_dimension=0,
        tiled=True,
    ).astype(jnp.float32)
    return (residual.astype(jnp.float32) + channel_sum).astype(jnp.bfloat16)


MESH = pl.DeviceIdType.MESH
Y_SIZE = 2
MIX_GROUPS = 4
DOWN_GROUPS = 8
DIRECT = (7,)


def fits(mesh):
    n_fs, n_tp = mesh.shape["fs"], mesh.shape["tp"]
    return n_tp == 2 * Y_SIZE and n_fs == 4 * Y_SIZE


def shifted_down(values, by, fill):
    if by % 8 == 0:
        top = jnp.full((by, values.shape[1]), fill, values.dtype)
        return jnp.concatenate([top, values[: values.shape[0] - by]], axis=0)
    rows = lax.broadcasted_iota(jnp.int32, values.shape, 0)
    return jnp.where(rows < by, fill, pltpu.roll(values, by, 0))


def one_minus_exp(exponent):
    series = 1.0
    for order in range(8, 1, -1):
        series = 1.0 + exponent * (1.0 / order) * series
    return jnp.where(exponent > -0.35, -exponent * series, 1.0 - jnp.exp(exponent))


def fused(
    nz,
    tok_in, scale1, wb, wg, taps, rblk, iblk, logits, extra_in, wo, scale2, wu, wd,
    out,
    normed, fb, fg, fo, fu, fd, rdiag, idiag, tok, extra,
    part1, pair1, give1, got1, res, mid, hidden,
    part2, pair2, agive, agot, bgive, bgot,
    z_send, y_send, w_recv, r_send, r_recv, a_send, a_recv, b_send, b_recv, l_sem,
):
    f = lax.axis_index("fs")
    t = lax.axis_index("tp")
    z, y = f // Y_SIZE, f % Y_SIZE
    x, c = t // 2, t % 2
    last = nz - 1
    parity = z % 2
    at_end = (z == 0) | (z == last)
    zmate = z + 1 - 2 * parity
    ymate = z * Y_SIZE + (1 - y)
    xmate = (1 - x) * 2 + c
    cmate = x * 2 + (1 - c)
    diagonal = (1 - x) * 2 + (1 - c)
    rows, width = tok.shape
    own_rows = out.shape[0]
    depth = wb.shape[0]
    half = depth // 2
    units = fu.shape[1]

    early = [
        pltpu.make_async_copy(tok_in, tok, l_sem.at[0]),
        pltpu.make_async_copy(extra_in, extra, l_sem.at[1]),
    ]
    for copy in early:
        copy.start()
    barrier = pltpu.get_barrier_semaphore()
    for k in range(1, nz):
        other = lax.rem(z + k, nz) * Y_SIZE + y
        pl.semaphore_signal(barrier, inc=1, device_id={"fs": other, "tp": t}, device_id_type=MESH)
    pl.semaphore_signal(barrier, inc=1, device_id={"fs": ymate, "tp": t}, device_id_type=MESH)
    for other in (xmate, cmate):
        pl.semaphore_signal(barrier, inc=1, device_id={"fs": f, "tp": other}, device_id_type=MESH)
    to_d = {"fs": zmate * Y_SIZE + y, "tp": xmate}
    pl.semaphore_signal(barrier, inc=1, device_id=to_d, device_id_type=MESH)
    pl.semaphore_wait(barrier, nz + 3)

    sent = []

    def start(pred, copy):
        if pred is None:
            copy.start()
        else:
            pl.when(pred)(copy.start)
        sent.append((pred, copy))

    plain = (wb, wg, wo)
    whole = (fb, fg, fo)

    def source(g, way_parity):
        if g < 3:
            return plain[g]
        w = wu if g < 5 else wd
        first = half * ((g - 3) % 2)
        return w.at[
            pl.ds(first, half), pl.ds(pl.multiple_of(way_parity * units, units), units)
        ]

    def slot(g, zs, ys):
        if g < 3:
            return whole[g].at[pl.ds(pl.multiple_of((zs * Y_SIZE + ys) * depth, depth), depth), :]
        if g < 5:
            at = (zs * Y_SIZE + ys) * depth + (g - 3) * half
            return fu.at[pl.ds(pl.multiple_of(at, half), half), :]
        at = ((zs * 2 + (g - 5)) * Y_SIZE + ys) * half
        return fd.at[pl.ds(pl.multiple_of(at, half), half), :]

    def z_copy(g, src, zs, zt, index):
        return pltpu.make_async_remote_copy(
            src_ref=src,
            dst_ref=slot(g, zs, y),
            send_sem=z_send.at[g, index],
            recv_sem=w_recv.at[g, zs * Y_SIZE + y],
            device_id={"fs": zt * Y_SIZE + y, "tp": t},
            device_id_type=MESH,
        )

    def y_copy(g, src, zs):
        return pltpu.make_async_remote_copy(
            src_ref=src,
            dst_ref=slot(g, zs, y),
            send_sem=y_send.at[g, zs],
            recv_sem=w_recv.at[g, zs * Y_SIZE + y],
            device_id={"fs": ymate, "tp": t},
            device_id_type=MESH,
        )

    def take(g, zs, ys):
        here = slot(g, zs, ys)
        pltpu.make_async_remote_copy(
            src_ref=here,
            dst_ref=here,
            send_sem=y_send.at[g, zs],
            recv_sem=w_recv.at[g, zs * Y_SIZE + ys],
            device_id={"fs": ymate, "tp": t},
            device_id_type=MESH,
        ).wait_recv()

    def spread_z(g, outer=None, far=range(1, nz), held=None):
        for d in (1,) if g < 3 else far:
            for way in (0, 1):
                zt = z + d if way == 0 else z - d
                exists = zt <= last if way == 0 else zt >= 0
                if outer is not None:
                    to_end = (zt == 0) | (zt == last)
                    exists = exists & (to_end if outer else jnp.logical_not(to_end))
                if held is not None:
                    exists = exists & (at_end if held else jnp.logical_not(at_end))
                start(exists, z_copy(g, source(g, lax.rem(zt + nz, 2)), z, zt, (d - 1) * 2 + way))

    def own(g):
        start(None, y_copy(g, source(g, parity), z))

    def forward(g, d):
        for way in (0, 1):
            zs = z - d if way == 0 else z + d
            exists = zs >= 0 if way == 0 else zs <= last
            pl.when(exists)(functools.partial(take, g, zs, y))
            if d < last:
                onward = z < last if way == 0 else z > 0
                zt = z + 1 if way == 0 else z - 1
                start(exists & onward, z_copy(g, slot(g, zs, y), zs, zt, d * 2 + way))
            start(exists, y_copy(g, slot(g, zs, y), zs))

    side = z // (nz // 2)
    origins = [zmate] + [rank + side * (last - 2 * rank) for rank in range(2, nz)]

    def hand_over(g, k):
        take(g, origins[k], y)
        start(None, y_copy(g, slot(g, origins[k], y), origins[k]))

    def take_across(g):
        for zs in range(nz):
            take(g, zs, 1 - y)

    def near_copy(src, dst, device, index, send, recv):
        copy = pltpu.make_async_remote_copy(
            src_ref=src,
            dst_ref=dst,
            send_sem=send.at[index],
            recv_sem=recv.at[index],
            device_id=device,
            device_id_type=MESH,
        )
        copy.start()
        sent.append((None, copy))
        return copy

    to_x = {"fs": f, "tp": xmate}
    to_c = {"fs": f, "tp": cmate}
    to_z = {"fs": zmate * Y_SIZE + y, "tp": t}

    spread_z(0)
    own(0)
    spread_z(1)
    own(1)

    stays = [
        pltpu.make_async_copy(source(g, parity), slot(g, z, y), l_sem.at[2 + g]) for g in range(7)
    ]
    for copy in stays:
        copy.start()
    block = rblk.shape[1]
    for blocks, diag in ((rblk, rdiag), (iblk, idiag)):
        diag[...] = jnp.zeros_like(diag)
        for b in range(rblk.shape[0]):
            diag[b * block : (b + 1) * block, b * block : (b + 1) * block] = blocks[b]

    for copy in early:
        copy.wait()

    def norm_rows(i, carry):
        at = pl.ds(pl.multiple_of(i * 32, 32), 32)
        normed[at, :] = rms_scaled(tok[at, :], scale1[...])
        return carry

    lax.fori_loop(0, rows // 32, norm_rows, 0)

    forward(0, 1)
    forward(1, 1)
    forward(0, 2)
    own(2)
    forward(1, 2)
    spread_z(2)
    forward(0, 3)
    forward(1, 3)
    forward(2, 1)
    spread_z(3, False)
    spread_z(4, False)
    for copy in stays:
        copy.wait()
    take_across(0)

    branch = jnp.dot(normed[...], fb[...], preferred_element_type=jnp.float32)
    branch = branch.astype(jnp.bfloat16).astype(jnp.float32)
    tap_count = taps.shape[0]
    running = branch * taps[tap_count - 1 : tap_count, :].astype(jnp.float32)
    for offset in range(tap_count - 1):
        by = tap_count - 1 - offset
        running = running + shifted_down(branch, by, 0.0) * taps[offset : offset + 1, :].astype(
            jnp.float32
        )
    convolved = running.astype(jnp.bfloat16)
    rate = jax.nn.sigmoid(jnp.dot(convolved, rdiag[...], preferred_element_type=jnp.float32))
    admission = jax.nn.sigmoid(jnp.dot(convolved, idiag[...], preferred_element_type=jnp.float32))
    base = -jnp.log1p(jnp.exp(-logits[...]))
    log_keep = decay_rate_scale * rate * base + extra[...]
    keep = jnp.exp(log_keep)
    memory = jnp.sqrt(one_minus_exp(2.0 * log_keep)) * (admission * convolved.astype(jnp.float32))
    by = 1
    while by < rows:
        memory = keep * shifted_down(memory, by, 0.0) + memory
        if 2 * by < rows:
            keep = keep * shifted_down(keep, by, 1.0)
        by *= 2
    forward(2, 2)
    take_across(1)
    gate = jnp.dot(normed[...], fg[...], preferred_element_type=jnp.float32)
    gate = gate.astype(jnp.bfloat16).astype(jnp.float32)
    recurrent = (memory * jax.nn.gelu(gate)).astype(jnp.bfloat16)

    forward(2, 3)
    spread_z(3, True)
    spread_z(4, True)
    spread_z(5, False, held=False)
    spread_z(6, False, held=False)
    own(3)
    own(4)

    inner = z + side * (last - 2 * z)
    ranks = [inner, 1 - inner] + list(range(2, nz))
    order = [rank + side * (last - 2 * rank) for rank in ranks]
    span = width // MIX_GROUPS
    own_at = pl.ds(pl.multiple_of(t * own_rows, own_rows), own_rows)
    firsts, seconds = [], []

    def mix_columns(j):
        return pl.ds(pl.multiple_of(order[j] * span, span), span)

    def mix_first(j):
        firsts[j].wait_recv()
        away = part1[j, 1 - x, c].astype(jnp.float32) + pair1[j, 1 - x].astype(jnp.float32)
        give1[j] = away.astype(jnp.bfloat16)
        seconds.append(
            near_copy(give1.at[j], got1.at[j], to_x, MIX_GROUPS + j, r_send, r_recv)
        )

    def mix_second(j):
        seconds[j].wait_recv()
        mixed = part1[j, x, c].astype(jnp.float32) + pair1[j, x].astype(jnp.float32)
        mixed = mixed + got1[j].astype(jnp.float32)
        at = mix_columns(j)
        res[:, at] = (tok[own_at, at].astype(jnp.float32) + mixed).astype(jnp.bfloat16)

    for j in range(MIX_GROUPS):
        if j == 2:
            mix_first(1)
        take(2, order[j], 1 - y)
        product = contract_columns(recurrent, fo[mix_columns(j), :])
        part1[j] = product.astype(jnp.bfloat16).reshape(2, 2, own_rows, span)
        firsts.append(
            near_copy(part1.at[j, :, 1 - c], pair1.at[j], to_c, j, r_send, r_recv)
        )
        if j == 1:
            mix_first(0)
        if j > 1:
            mix_first(j)
    for j in range(MIX_GROUPS):
        mix_second(j)

    mid[parity, t] = rms_scaled(res[...], scale2[...])
    mine = mid.at[parity, t]
    theirs = mid.at[1 - parity, t]
    near_copy(mine, mine, to_x, 1, a_send, a_recv)
    near_copy(mine, mine, to_z, 0, a_send, a_recv)
    near_copy(mine, mine, to_c, 2, a_send, a_recv)
    spread_z(5, False, held=True)
    spread_z(6, False, held=True)
    spread_z(5, True, (1,))
    spread_z(6, True, (1,))

    def arrived(here, index):
        pltpu.make_async_remote_copy(
            src_ref=here,
            dst_ref=here,
            send_sem=a_send.at[index],
            recv_sem=a_recv.at[index],
            device_id=to_c,
            device_id_type=MESH,
        ).wait_recv()

    def pass_on(here, device, index):
        near_copy(here, here, device, index, a_send, a_recv)

    beside = mid.at[parity, xmate]
    across = mid.at[1 - parity, xmate]
    for k in range(nz - 1):
        hand_over(3, k)
    for k in range(nz - 1):
        hand_over(4, k)
    own(5)
    own(6)
    arrived(beside, 1)
    pass_on(beside, to_c, 5)
    arrived(theirs, 0)
    pass_on(theirs, to_x, 3)
    pass_on(theirs, to_c, 4)
    spread_z(5, True, range(2, nz))
    spread_z(6, True, range(2, nz))
    arrived(mid.at[parity, cmate], 2)
    arrived(mid.at[parity, diagonal], 5)
    take_across(3)
    take_across(4)

    tile = 256

    def up(par):
        def up_tile(i, carry):
            at = pl.ds(pl.multiple_of(i * tile, tile), tile)
            raised = jnp.dot(
                mid[par].reshape(rows, width), fu[:, at], preferred_element_type=jnp.float32
            )
            hidden[par, :, at] = jnp.square(jnp.maximum(raised, 0.0)).astype(jnp.bfloat16)
            return carry

        lax.fori_loop(0, units // tile, up_tile, 0)

    up(parity)
    hand_over(5, 0)
    arrived(across, 3)
    pass_on(across, to_c, 6)
    arrived(mid.at[1 - parity, cmate], 4)
    arrived(mid.at[1 - parity, diagonal], 6)
    up(1 - parity)

    narrow = width // DOWN_GROUPS
    exchanges = [[], [], []]

    turns = [(1, 0), (0, 0), (1, 1), (0, 1)]
    turns += [(rank, k) for k in range(2) for rank in range(2, nz)]

    def place(j):
        rank = turns[j][0]
        return rank + side * (last - 2 * rank)

    def pair_sum(j, par, xs):
        return part2[j, par, xs, c].astype(jnp.float32) + pair2[j, par, xs].astype(jnp.float32)

    def x_first(j):
        return j not in (4, 6)

    def down_out(j, total):
        for ys in range(Y_SIZE):
            first = (place(j) * Y_SIZE + ys) * depth + turns[j][1] * half
            at = pl.ds(pl.multiple_of(first, half), half)
            out[:, at] = (
                res[:, at].astype(jnp.float32) + total[:, ys * half : (ys + 1) * half]
            ).astype(jnp.bfloat16)

    def down_direct(j):
        exchanges[0][j].wait_recv()
        agive[j, 0] = pair_sum(j, parity, 1 - x).astype(jnp.bfloat16)
        agive[j, 1] = pair_sum(j, 1 - parity, x).astype(jnp.bfloat16)
        bgive[j] = pair_sum(j, 1 - parity, 1 - x).astype(jnp.bfloat16)
        trio = [
            (bgive.at[j], bgot.at[j], to_d, 3),
            (agive.at[j, 0], agot.at[j, 0], to_x, 1),
            (agive.at[j, 1], agot.at[j, 1], to_z, 2),
        ]
        exchanges[1].append(
            [near_copy(a, b, dev, k * DOWN_GROUPS + j, b_send, b_recv) for a, b, dev, k in trio]
        )

    def down_last(j):
        for copy in exchanges[1][j]:
            copy.wait_recv()
        total = pair_sum(j, parity, x) + bgot[j].astype(jnp.float32)
        total = total + agot[j, 0].astype(jnp.float32) + agot[j, 1].astype(jnp.float32)
        down_out(j, total)

    def down_first(j):
        if j in DIRECT:
            return down_direct(j)
        exchanges[0][j].wait_recv()
        for k in range(2):
            away = pair_sum(j, k, 1 - x) if x_first(j) else pair_sum(j, 1 - parity, k)
            agive[j, k] = away.astype(jnp.bfloat16)
        device = to_x if x_first(j) else to_z
        exchanges[1].append(
            near_copy(agive.at[j], agot.at[j], device, DOWN_GROUPS + j, b_send, b_recv)
        )

    def down_second(j):
        if j in DIRECT:
            exchanges[2].append(None)
            return
        exchanges[1][j].wait_recv()
        if x_first(j):
            total = pair_sum(j, 1 - parity, x) + agot[j, 1 - parity].astype(jnp.float32)
        else:
            total = pair_sum(j, parity, 1 - x) + agot[j, 1 - x].astype(jnp.float32)
        bgive[j] = total.astype(jnp.bfloat16)
        device = to_z if x_first(j) else to_x
        exchanges[2].append(
            near_copy(bgive.at[j], bgot.at[j], device, 2 * DOWN_GROUPS + j, b_send, b_recv)
        )

    def down_third(j):
        if j in DIRECT:
            return down_last(j)
        exchanges[2][j].wait_recv()
        total = pair_sum(j, parity, x) + bgot[j].astype(jnp.float32)
        total = total + agot[j, parity if x_first(j) else x].astype(jnp.float32)
        down_out(j, total)

    ahead = {0: [(6, 0)], 1: [(5, 1)], 2: [(5, 2)], 3: [(6, 1)], 4: [(6, 2)]}
    for j in range(DOWN_GROUPS):
        for step in ahead.get(j, []):
            hand_over(*step)
        q = place(j)
        take(5 + turns[j][1], q, 1 - y)
        at = pl.ds(pl.multiple_of((q * 2 + turns[j][1]) * narrow, narrow), narrow)
        product = contract_columns(hidden[...].reshape(2 * rows, units), fd[at, :])
        part2[j] = product.astype(jnp.bfloat16).reshape(2, 2, 2, own_rows, narrow)
        exchanges[0].append(
            near_copy(part2.at[j, :, :, 1 - c], pair2.at[j], to_c, j, b_send, b_recv)
        )
        if j > 0:
            down_first(j - 1)
        if j > 2:
            down_second(j - 3)
        if j > 5:
            down_third(j - 6)
    down_first(DOWN_GROUPS - 1)
    down_second(DOWN_GROUPS - 3)
    down_second(DOWN_GROUPS - 2)
    down_third(DOWN_GROUPS - 6)
    down_second(DOWN_GROUPS - 1)
    for j in range(DOWN_GROUPS - 5, DOWN_GROUPS):
        down_third(j)

    for pred, copy in sent:
        if pred is None:
            copy.wait_send()
        else:
            pl.when(pred)(copy.wait_send)


def fused_local(
    mesh,
    tokens,
    first_norm_scale,
    recurrent_branch_matrix,
    gelu_gate_matrix,
    filter_taps_weight,
    recurrence_gate_blocks,
    input_gate_blocks,
    base_decay_logits,
    extra_log_decay,
    mixer_output_matrix,
    second_norm_scale,
    mixer_up_matrix,
    mixer_down_matrix,
):
    n_fs, n_tp = mesh.shape["fs"], mesh.shape["tp"]
    rows, width = tokens.shape
    own_rows = rows // n_tp
    channels = recurrent_branch_matrix.shape[1]
    units = mixer_up_matrix.shape[1] // 2
    span = width // MIX_GROUPS
    narrow = width // DOWN_GROUPS
    low, high = jnp.bfloat16, jnp.float32
    vmem = pl.BlockSpec(memory_space=pltpu.VMEM)
    hbm = pl.BlockSpec(memory_space=pl.ANY)
    return pl.pallas_call(
        functools.partial(fused, n_fs // Y_SIZE),
        out_shape=jax.ShapeDtypeStruct((own_rows, width), low),
        in_specs=[hbm, vmem, hbm, hbm] + [vmem] * 4 + [hbm, hbm, vmem, hbm, hbm],
        out_specs=vmem,
        scratch_shapes=[
            pltpu.VMEM((rows, width), low),
            pltpu.VMEM((width, channels), low),
            pltpu.VMEM((width, channels), low),
            pltpu.VMEM((width, channels), low),
            pltpu.VMEM((width, units), low),
            pltpu.VMEM((width, units), low),
            pltpu.VMEM((channels, channels), low),
            pltpu.VMEM((channels, channels), low),
            pltpu.VMEM((rows, width), low),
            pltpu.VMEM((rows, channels), high),
            pltpu.VMEM((MIX_GROUPS, 2, 2, own_rows, span), low),
            pltpu.VMEM((MIX_GROUPS, 2, own_rows, span), low),
            pltpu.VMEM((MIX_GROUPS, own_rows, span), low),
            pltpu.VMEM((MIX_GROUPS, own_rows, span), low),
            pltpu.VMEM((own_rows, width), low),
            pltpu.VMEM((2, n_tp, own_rows, width), low),
            pltpu.VMEM((2, rows, units), low),
            pltpu.VMEM((DOWN_GROUPS, 2, 2, 2, own_rows, narrow), low),
            pltpu.VMEM((DOWN_GROUPS, 2, 2, own_rows, narrow), low),
            pltpu.VMEM((DOWN_GROUPS, 2, own_rows, narrow), low),
            pltpu.VMEM((DOWN_GROUPS, 2, own_rows, narrow), low),
            pltpu.VMEM((DOWN_GROUPS, own_rows, narrow), low),
            pltpu.VMEM((DOWN_GROUPS, own_rows, narrow), low),
            pltpu.SemaphoreType.DMA((7, 6)),
            pltpu.SemaphoreType.DMA((7, n_fs // Y_SIZE)),
            pltpu.SemaphoreType.DMA((7, n_fs)),
            pltpu.SemaphoreType.DMA((2 * MIX_GROUPS,)),
            pltpu.SemaphoreType.DMA((2 * MIX_GROUPS,)),
            pltpu.SemaphoreType.DMA((9,)),
            pltpu.SemaphoreType.DMA((9,)),
            pltpu.SemaphoreType.DMA((4 * DOWN_GROUPS,)),
            pltpu.SemaphoreType.DMA((4 * DOWN_GROUPS,)),
            pltpu.SemaphoreType.DMA((9,)),
        ],
        compiler_params=pltpu.CompilerParams(
            collective_id=0, has_side_effects=True, vmem_limit_bytes=60 * 1024 * 1024
        ),
        name="fused_layer",
    )(
        tokens,
        first_norm_scale.reshape(1, width),
        recurrent_branch_matrix,
        gelu_gate_matrix,
        filter_taps_weight,
        recurrence_gate_blocks,
        input_gate_blocks,
        base_decay_logits.reshape(1, channels),
        extra_log_decay,
        mixer_output_matrix,
        second_norm_scale.reshape(1, width),
        mixer_up_matrix,
        mixer_down_matrix,
    )


def solution(mesh):
    in_specs = (
        P("fs", None),
        P(),
        P("fs", "tp"),
        P("fs", "tp"),
        P(None, "tp"),
        P("tp", None, None),
        P("tp", None, None),
        P("tp"),
        P("fs", "tp"),
        P("fs", "tp"),
        P(),
        P("fs", "tp"),
        P("fs", "tp"),
    )
    out_specs = P(("fs", "tp"), None)
    body = functools.partial(fused_local, mesh) if fits(mesh) else local
    return jax.shard_map(body, mesh=mesh, in_specs=in_specs, out_specs=out_specs, check_vma=False)
```

```python
import functools

import jax
import jax.numpy as jnp
from jax import lax
from jax.experimental import pallas as pl
from jax.experimental.pallas import tpu as pltpu
from jax.sharding import PartitionSpec as P

epsilon = 1e-06
decay_rate_scale = 8.0


def rms_scaled(sequence_token_rows, scales):
    widened = sequence_token_rows.astype(jnp.float32)
    mean_square = jnp.mean(widened * widened, axis=-1, keepdims=True)
    return (widened * lax.rsqrt(mean_square + epsilon) * scales).astype(jnp.bfloat16)


def linear_combine(earlier, later):
    return (earlier[0] * later[0], later[0] * earlier[1] + later[1])


def causal_taps(branch, filter_taps_weight):
    tap_count = filter_taps_weight.shape[0]
    positions = branch.shape[0]
    padded = jnp.pad(branch.astype(jnp.float32), ((tap_count - 1, 0), (0, 0)))
    running = jnp.zeros(branch.shape, jnp.float32)
    for offset in range(tap_count):
        running = running + padded[offset : offset + positions] * filter_taps_weight[offset].astype(
            jnp.float32
        )
    return running.astype(jnp.bfloat16)


def block_map(convolved, blocks):
    positions, channels = convolved.shape
    grouped = convolved.reshape(positions, blocks.shape[0], blocks.shape[1])
    mapped = jnp.einsum("sgi,gij->sgj", grouped, blocks, preferred_element_type=jnp.float32)
    return jax.nn.sigmoid(mapped.reshape(positions, channels))


def contract_columns(left, right):
    return lax.dot_general(
        left, right, (((1,), (1,)), ((), ())), preferred_element_type=jnp.float32
    )


def local(
    tokens,
    first_norm_scale,
    recurrent_branch_matrix,
    gelu_gate_matrix,
    filter_taps_weight,
    recurrence_gate_blocks,
    input_gate_blocks,
    base_decay_logits,
    extra_log_decay,
    mixer_output_matrix,
    second_norm_scale,
    mixer_up_matrix,
    mixer_down_matrix,
):
    positions = tokens.shape[0]
    own_count = positions // lax.axis_size("tp")
    normed = rms_scaled(tokens, first_norm_scale)
    branch_sum = jnp.dot(
        normed,
        lax.all_gather(recurrent_branch_matrix, "fs", axis=0, tiled=True),
        preferred_element_type=jnp.float32,
    )
    gate_sum = jnp.dot(
        normed,
        lax.all_gather(gelu_gate_matrix, "fs", axis=0, tiled=True),
        preferred_element_type=jnp.float32,
    )
    branch = branch_sum.astype(jnp.bfloat16)
    gate_branch = gate_sum.astype(jnp.bfloat16)
    out_full = lax.all_gather(mixer_output_matrix, "fs", axis=0, tiled=True)
    convolved = causal_taps(branch, filter_taps_weight)
    recurrence_gate_value = block_map(convolved, recurrence_gate_blocks)
    admission = block_map(convolved, input_gate_blocks)
    log_keep_factor = (
        decay_rate_scale * recurrence_gate_value * jax.nn.log_sigmoid(base_decay_logits)
        + extra_log_decay
    )
    retain = jnp.exp(log_keep_factor)
    driven = jnp.sqrt(-jnp.expm1(2.0 * log_keep_factor)) * (
        admission * convolved.astype(jnp.float32)
    )
    memory = lax.associative_scan(linear_combine, (retain, driven), axis=0)[1]
    recurrent = (memory * jax.nn.gelu(gate_branch.astype(jnp.float32))).astype(jnp.bfloat16)
    up_full = lax.all_gather(mixer_up_matrix, "fs", axis=0, tiled=True)
    whole_sum = lax.psum(contract_columns(recurrent, out_full).astype(jnp.bfloat16), "tp").astype(
        jnp.float32
    )
    residual_all = (tokens.astype(jnp.float32) + whole_sum).astype(jnp.bfloat16)
    raised = jnp.dot(
        rms_scaled(residual_all, second_norm_scale), up_full, preferred_element_type=jnp.float32
    )
    hidden = jnp.square(jax.nn.relu(raised)).astype(jnp.bfloat16)
    residual = lax.dynamic_slice_in_dim(
        residual_all, lax.axis_index("tp") * own_count, own_count, 0
    )
    down_full = lax.all_gather(mixer_down_matrix, "fs", axis=0, tiled=True)
    channel_sum = lax.psum_scatter(
        contract_columns(hidden, down_full).astype(jnp.bfloat16),
        "tp",
        scatter_dimension=0,
        tiled=True,
    ).astype(jnp.float32)
    return (residual.astype(jnp.float32) + channel_sum).astype(jnp.bfloat16)


MESH = pl.DeviceIdType.MESH
Y_SIZE = 2
MIX_GROUPS = 4
DOWN_GROUPS = 8


def fits(mesh):
    n_fs, n_tp = mesh.shape["fs"], mesh.shape["tp"]
    return n_tp == 2 * Y_SIZE and n_fs == 4 * Y_SIZE


def shifted_down(values, by, fill):
    if by % 8 == 0:
        top = jnp.full((by, values.shape[1]), fill, values.dtype)
        return jnp.concatenate([top, values[: values.shape[0] - by]], axis=0)
    rows = lax.broadcasted_iota(jnp.int32, values.shape, 0)
    return jnp.where(rows < by, fill, pltpu.roll(values, by, 0))


def one_minus_exp(exponent):
    series = 1.0
    for order in range(8, 1, -1):
        series = 1.0 + exponent * (1.0 / order) * series
    return jnp.where(exponent > -0.35, -exponent * series, 1.0 - jnp.exp(exponent))


def fused(
    nz,
    tok_in, scale1_in, wb, wg, taps_in, rblk_in, iblk_in, logits_in, extra_in, wo, scale2_in, wu, wd,
    result,
    scale1, taps, rblk, iblk, logits, scale2,
    normed, fb, fg, fo, fu, fd, rdiag, idiag, tok, extra,
    part1, pair1, give1, got1, res, mid, hidden,
    part2, pair2, give2, got2, tally,
    s_sem, along, lump, across, r_recv, a_recv, b_recv, l_sem,
):
    f = lax.axis_index("fs")
    t = lax.axis_index("tp")
    z, y = f // Y_SIZE, f % Y_SIZE
    x, c = t // 2, t % 2
    last = nz - 1
    parity = z % 2
    at_end = (z == 0) | (z == last)
    zmate = z + 1 - 2 * parity
    ymate = z * Y_SIZE + (1 - y)
    xmate = (1 - x) * 2 + c
    cmate = x * 2 + (1 - c)
    diagonal = (1 - x) * 2 + (1 - c)
    rows, width = tok.shape
    own_rows = result.shape[0]
    depth = wb.shape[0]
    half = depth // 2
    units = fu.shape[1]

    barrier = pltpu.get_barrier_semaphore()

    def greet(sem, device):
        pl.semaphore_signal(sem, inc=1, device_id=device, device_id_type=MESH)

    to_x = {"fs": f, "tp": xmate}
    to_c = {"fs": f, "tp": cmate}
    to_z = {"fs": zmate * Y_SIZE + y, "tp": t}
    to_d = {"fs": zmate * Y_SIZE + y, "tp": xmate}
    inside = jnp.logical_not(at_end)
    for k in range(1, nz):
        greet(barrier, {"fs": lax.rem(z + k, nz) * Y_SIZE + y, "tp": t})
    for device in ({"fs": ymate, "tp": t}, to_x, to_c, to_d):
        greet(barrier, device)
    early = [
        pltpu.make_async_copy(given, kept, l_sem.at[1 + i])
        for i, (given, kept) in enumerate(
            (
                (tok_in, tok),
                (scale1_in, scale1),
                (rblk_in, rblk),
                (iblk_in, iblk),
                (taps_in, taps),
                (logits_in, logits),
                (extra_in, extra),
                (scale2_in, scale2),
            )
        )
    ]

    for copy in early:
        copy.start()
    pl.semaphore_wait(barrier, nz + 3)

    def start(pred, copy):
        if pred is None:
            copy.start()
        else:
            pl.when(pred)(copy.start)

    def settle(count, sem):
        lot = tally.at[pl.ds(0, count * 16), :]
        pltpu.make_async_copy(lot, lot, sem).wait()

    plain = (wb, wg, wo)
    whole = (fb, fg, fo)
    lumped, single = (0, 1, 3, 4), (2, 5, 6)

    def source(g, way_parity):
        if g < 3:
            return plain[g]
        w = wu if g < 5 else wd
        first = half * ((g - 3) % 2)
        return w.at[
            pl.ds(first, half), pl.ds(pl.multiple_of(way_parity * units, units), units)
        ]

    def slot(g, zs, ys):
        if g < 3:
            return whole[g].at[pl.ds(pl.multiple_of((zs * Y_SIZE + ys) * depth, depth), depth), :]
        if g < 5:
            at = (zs * Y_SIZE + ys) * depth + (g - 3) * half
            return fu.at[pl.ds(pl.multiple_of(at, half), half), :]
        at = ((zs * 2 + (g - 5)) * Y_SIZE + ys) * half
        return fd.at[pl.ds(pl.multiple_of(at, half), half), :]

    def over(g, zs):
        return lump.at[lumped.index(g)] if g in lumped else across.at[single.index(g), zs]

    def z_copy(g, src, zs, zt):
        return pltpu.make_async_remote_copy(
            src_ref=src,
            dst_ref=slot(g, zs, y),
            send_sem=s_sem.at[0 if g < 3 else 1],
            recv_sem=along.at[g, zs],
            device_id={"fs": zt * Y_SIZE + y, "tp": t},
            device_id_type=MESH,
        )

    def y_copy(g, src, zs):
        return pltpu.make_async_remote_copy(
            src_ref=src,
            dst_ref=slot(g, zs, y),
            send_sem=s_sem.at[2],
            recv_sem=over(g, zs),
            device_id={"fs": ymate, "tp": t},
            device_id_type=MESH,
        )

    def landed(here, sem):
        pltpu.make_async_copy(here, here, sem).wait()

    def take(g, zs):
        landed(slot(g, zs, y), along.at[g, zs])

    def spread_z(g, outer=None, far=range(1, nz), held=None):
        for d in (1,) if g < 3 else far:
            for way in (0, 1):
                zt = z + d if way == 0 else z - d
                exists = zt <= last if way == 0 else zt >= 0
                if outer is not None:
                    to_end = (zt == 0) | (zt == last)
                    exists = exists & (to_end if outer else jnp.logical_not(to_end))
                if held is not None:
                    exists = exists & (at_end if held else jnp.logical_not(at_end))
                start(exists, z_copy(g, source(g, lax.rem(zt + nz, 2)), z, zt))

    def own(g):
        start(None, y_copy(g, source(g, parity), z))

    def forward(g, d):
        for way in (0, 1):
            zs = z - d if way == 0 else z + d
            exists = zs >= 0 if way == 0 else zs <= last
            pl.when(exists)(functools.partial(take, g, zs))
            if d < last:
                onward = z < last if way == 0 else z > 0
                zt = z + 1 if way == 0 else z - 1
                start(exists & onward, z_copy(g, slot(g, zs, y), zs, zt))
            start(exists, y_copy(g, slot(g, zs, y), zs))

    side = z // (nz // 2)
    origins = [zmate] + [rank + side * (last - 2 * rank) for rank in range(2, nz)]

    def hand_over(g, k):
        take(g, origins[k])
        start(None, y_copy(g, slot(g, origins[k], y), origins[k]))

    def take_lump(g):
        count = nz * depth if g < 3 else nz * half
        landed((whole[g] if g < 3 else fu).at[pl.ds(0, count), :], over(g, 0))

    def take_over(g, zs):
        landed(slot(g, zs, 1 - y), over(g, zs))

    def near_copy(src, dst, device, sem):
        copy = pltpu.make_async_remote_copy(
            src_ref=src,
            dst_ref=dst,
            send_sem=s_sem.at[3],
            recv_sem=sem,
            device_id=device,
            device_id_type=MESH,
        )
        copy.start()
        return copy

    spread_z(0)
    own(0)
    spread_z(1)
    own(1)

    stays = [
        pltpu.make_async_copy(source(g, parity), slot(g, z, y), l_sem.at[0]) for g in range(7)
    ]
    for copy in stays:
        copy.start()
    for copy in early:
        copy.wait()
    block = rblk.shape[1]
    for blocks, diag in ((rblk, rdiag), (iblk, idiag)):
        diag[...] = jnp.zeros_like(diag)
        for b in range(rblk.shape[0]):
            diag[b * block : (b + 1) * block, b * block : (b + 1) * block] = blocks[b]

    def norm_rows(i, carry):
        at = pl.ds(pl.multiple_of(i * 32, 32), 32)
        normed[at, :] = rms_scaled(tok[at, :], scale1[...])
        return carry

    lax.fori_loop(0, rows // 32, norm_rows, 0)

    forward(0, 1)
    forward(1, 1)
    forward(0, 2)
    own(2)
    forward(1, 2)
    spread_z(2)
    forward(0, 3)
    forward(1, 3)
    forward(2, 1)
    spread_z(3, False)
    spread_z(4, False)
    settle(depth // 16 * 7, l_sem.at[0])
    take_lump(0)

    branch = jnp.dot(normed[...], fb[...], preferred_element_type=jnp.float32)
    branch = branch.astype(jnp.bfloat16).astype(jnp.float32)
    tap_count = taps.shape[0]
    running = branch * taps[tap_count - 1 : tap_count, :].astype(jnp.float32)
    for offset in range(tap_count - 1):
        by = tap_count - 1 - offset
        running = running + shifted_down(branch, by, 0.0) * taps[offset : offset + 1, :].astype(
            jnp.float32
        )
    convolved = running.astype(jnp.bfloat16)
    rate = jax.nn.sigmoid(jnp.dot(convolved, rdiag[...], preferred_element_type=jnp.float32))
    admission = jax.nn.sigmoid(jnp.dot(convolved, idiag[...], preferred_element_type=jnp.float32))
    base = -jnp.log1p(jnp.exp(-logits[...]))
    log_keep = decay_rate_scale * rate * base + extra[...]
    keep = jnp.exp(log_keep)
    memory = jnp.sqrt(one_minus_exp(2.0 * log_keep)) * (admission * convolved.astype(jnp.float32))
    by = 1
    while by < rows:
        memory = keep * shifted_down(memory, by, 0.0) + memory
        if 2 * by < rows:
            keep = keep * shifted_down(keep, by, 1.0)
        by *= 2
    forward(2, 2)
    take_lump(1)
    gate = jnp.dot(normed[...], fg[...], preferred_element_type=jnp.float32)
    gate = gate.astype(jnp.bfloat16).astype(jnp.float32)
    recurrent = (memory * jax.nn.gelu(gate)).astype(jnp.bfloat16)

    forward(2, 3)
    spread_z(3, True)
    spread_z(4, True)
    spread_z(5, False, held=False)
    spread_z(6, False, held=False)
    own(3)
    own(4)

    inner = z + side * (last - 2 * z)
    ranks = [inner, 1 - inner] + list(range(2, nz))
    order = [rank + side * (last - 2 * rank) for rank in ranks]
    span = width // MIX_GROUPS
    own_at = pl.ds(pl.multiple_of(t * own_rows, own_rows), own_rows)
    firsts, seconds = [], []

    def mix_columns(j):
        return pl.ds(pl.multiple_of(order[j] * span, span), span)

    def mix_first(j):
        firsts[j].wait_recv()
        away = part1[j, 1 - x, c].astype(jnp.float32) + pair1[j, 1 - x].astype(jnp.float32)
        give1[j] = away.astype(jnp.bfloat16)
        seconds.append(
            near_copy(give1.at[j], got1.at[j], to_x, r_recv.at[MIX_GROUPS + j])
        )

    def mix_second(j):
        seconds[j].wait_recv()
        mixed = part1[j, x, c].astype(jnp.float32) + pair1[j, x].astype(jnp.float32)
        mixed = mixed + got1[j].astype(jnp.float32)
        at = mix_columns(j)
        res[:, at] = (tok[own_at, at].astype(jnp.float32) + mixed).astype(jnp.bfloat16)

    for j in range(MIX_GROUPS):
        if j == 2:
            mix_first(1)
        take_over(2, order[j])
        product = contract_columns(recurrent, fo[mix_columns(j), :])
        part1[j] = product.astype(jnp.bfloat16).reshape(2, 2, own_rows, span)
        firsts.append(
            near_copy(part1.at[j, :, 1 - c], pair1.at[j], to_c, r_recv.at[j])
        )
        if j == 1:
            mix_first(0)
        if j > 1:
            mix_first(j)
    for j in range(MIX_GROUPS):
        mix_second(j)

    mid[parity, t] = rms_scaled(res[...], scale2[...])
    mine = mid.at[parity, t]
    theirs = mid.at[1 - parity, t]
    near_copy(mine, mine, to_x, a_recv.at[1])
    near_copy(mine, mine, to_z, a_recv.at[0])
    near_copy(mine, mine, to_c, a_recv.at[2])
    spread_z(5, False, held=True)
    spread_z(6, False, held=True)
    spread_z(5, True, (1,))
    spread_z(6, True, (1,))

    def arrived(here, index):
        landed(here, a_recv.at[index])

    def pass_on(here, device, index):
        near_copy(here, here, device, a_recv.at[index])

    beside = mid.at[parity, xmate]
    askew = mid.at[1 - parity, xmate]
    for k in range(nz - 1):
        hand_over(3, k)
    for k in range(nz - 1):
        hand_over(4, k)
    own(5)
    own(6)
    arrived(beside, 1)
    pass_on(beside, to_c, 5)
    arrived(theirs, 0)
    pass_on(theirs, to_x, 3)
    pass_on(theirs, to_c, 4)
    spread_z(5, True, range(2, nz))
    spread_z(6, True, range(2, nz))
    arrived(mid.at[parity, cmate], 2)
    arrived(mid.at[parity, diagonal], 5)
    take_lump(3)
    take_lump(4)

    tile = 256

    def up(par):
        def up_tile(i, carry):
            at = pl.ds(pl.multiple_of(i * tile, tile), tile)
            raised = jnp.dot(
                mid[par].reshape(rows, width), fu[:, at], preferred_element_type=jnp.float32
            )
            hidden[par, :, at] = jnp.square(jnp.maximum(raised, 0.0)).astype(jnp.bfloat16)
            return carry

        lax.fori_loop(0, units // tile, up_tile, 0)

    up(parity)
    hand_over(5, 0)
    arrived(askew, 3)
    pass_on(askew, to_c, 6)
    arrived(mid.at[1 - parity, cmate], 4)
    arrived(mid.at[1 - parity, diagonal], 6)
    up(1 - parity)

    narrow = width // DOWN_GROUPS
    halves = [k for r in range(2) for k in range(2)] + [k for k in range(2) for r in range(2, nz)]
    final = DOWN_GROUPS - 1
    lots = [(j, None) for j in range(final - 1)] + [(final, 0), (final - 1, None), (final, 1)]
    shared, spread = {}, {}
    level = jnp.where(at_end, 0, 1)

    def number(lot):
        j, which = lot
        if j >= 4:
            return j + (which or 0)
        return (level if j < 2 else 1 - level) * 2 + j % 2

    def place(j):
        if j < 4:
            return z if j < 2 else zmate
        rank = 2 + (j - 4) % (nz - 2)
        return rank + side * (last - 2 * rank)

    def signal_at(lot, k):
        return b_recv.at[number(lot), k]

    def lot_columns(lot):
        which = lot[1]
        return pl.ds(0, narrow if which is None else half)

    def lot_sides(lot):
        which = lot[1]
        return list(range(Y_SIZE)) if which is None else [y if which == 0 else 1 - y]

    def pair_sum(lot, par, xs):
        at = lot_columns(lot)
        mine = part2[number(lot), par, xs, c, :, at].astype(jnp.float32)
        return mine + pair2[number(lot), par, xs, :, at].astype(jnp.float32)

    def multiply(i):
        lot = lots[i]
        j, which = lot
        q = place(j)
        if which != 0:
            take_over(5 + halves[j], q)
        first = (q * 2 + halves[j]) * narrow
        if which is not None:
            first = first + lot_sides(lot)[0] * half
        at = lot_columns(lot)
        some = fd[pl.ds(pl.multiple_of(first, half), at.size), :]
        product = contract_columns(hidden[...].reshape(2 * rows, units), some)
        n = number(lot)
        part2[n, :, :, :, :, at] = product.astype(jnp.bfloat16).reshape(2, 2, 2, own_rows, at.size)
        shared[lot] = near_copy(
            part2.at[n, :, :, 1 - c, :, at], pair2.at[n, :, :, :, at], to_c, signal_at(lot, 0)
        )

    def exchange(i):
        lot = lots[i]
        shared[lot].wait_recv()
        at = lot_columns(lot)
        ways = [
            (to_d, 1 - parity, 1 - x),
            (to_x, parity, 1 - x),
            (to_z, 1 - parity, x),
        ]
        spread[lot] = []
        for k, (device, par, xs) in enumerate(ways):
            n = number(lot)
            give2[n, k, :, at] = pair_sum(lot, par, xs).astype(jnp.bfloat16)
            spread[lot].append(
                near_copy(
                    give2.at[n, k, :, at], got2.at[n, k, :, at], device, signal_at(lot, k + 1)
                )
            )

    def finish(i):
        lot = lots[i]
        for copy in spread[lot]:
            copy.wait_recv()
        total = pair_sum(lot, parity, x)
        for k in range(3):
            total = total + got2[number(lot), k, :, lot_columns(lot)].astype(jnp.float32)
        for k, ys in enumerate(lot_sides(lot)):
            first = (place(lot[0]) * Y_SIZE + ys) * depth + halves[lot[0]] * half
            at = pl.ds(pl.multiple_of(first, half), half)
            result[:, at] = (
                res[:, at].astype(jnp.float32) + total[:, k * half : (k + 1) * half]
            ).astype(jnp.bfloat16)

    plan = [
        (hand_over, 6, 0),
        (multiply, 0),
        (multiply, 1),
        (exchange, 0),
        (exchange, 1),
        (multiply, 2),
        (hand_over, 5, 1),
        (exchange, 2),
        (hand_over, 5, 2),
        (multiply, 3),
        (exchange, 3),
        (multiply, 4),
        (exchange, 4),
        (hand_over, 6, 1),
        (multiply, 5),
        (exchange, 5),
        (hand_over, 6, 2),
        (multiply, 6),
        (exchange, 6),
        (multiply, 7),
        (exchange, 7),
        (multiply, 8),
        (exchange, 8),
        (finish, 0),
        (finish, 1),
        (finish, 2),
        (finish, 3),
        (finish, 4),
        (finish, 5),
        (finish, 6),
        (finish, 7),
        (finish, 8),
    ]
    for step, *which in plan:
        step(*which)
    pl.when(at_end)(functools.partial(settle, depth // 16 * 3, s_sem.at[0]))
    relayed = 3 * (2 + nz - 1)
    pl.when(inside)(functools.partial(settle, depth // 16 * relayed, s_sem.at[0]))
    settle(depth // 16 * 4 * (nz - 1), s_sem.at[1])
    settle(depth // 16 * 7 * nz, s_sem.at[2])
    bits = own_rows * width // (16 * depth)
    mixed = own_rows * span // (16 * depth)
    summed = own_rows * narrow // (16 * depth)
    settle(7 * bits + 3 * MIX_GROUPS * mixed + 7 * DOWN_GROUPS * summed, s_sem.at[3])


def fused_local(
    mesh,
    tokens,
    first_norm_scale,
    recurrent_branch_matrix,
    gelu_gate_matrix,
    filter_taps_weight,
    recurrence_gate_blocks,
    input_gate_blocks,
    base_decay_logits,
    extra_log_decay,
    mixer_output_matrix,
    second_norm_scale,
    mixer_up_matrix,
    mixer_down_matrix,
):
    n_fs, n_tp = mesh.shape["fs"], mesh.shape["tp"]
    rows, width = tokens.shape
    own_rows = rows // n_tp
    channels = recurrent_branch_matrix.shape[1]
    units = mixer_up_matrix.shape[1] // 2
    span = width // MIX_GROUPS
    narrow = width // DOWN_GROUPS
    low, high = jnp.bfloat16, jnp.float32
    hbm = pl.BlockSpec(memory_space=pl.ANY)
    return pl.pallas_call(
        functools.partial(fused, n_fs // Y_SIZE),
        out_shape=pltpu.VMEM((own_rows, width), low),
        in_specs=[hbm] * 13,
        out_specs=pl.BlockSpec(memory_space=pltpu.VMEM),
        scratch_shapes=[
            pltpu.VMEM((1, width), high),
            pltpu.VMEM(filter_taps_weight.shape, low),
            pltpu.VMEM(recurrence_gate_blocks.shape, low),
            pltpu.VMEM(input_gate_blocks.shape, low),
            pltpu.VMEM((1, channels), high),
            pltpu.VMEM((1, width), high),
            pltpu.VMEM((rows, width), low),
            pltpu.VMEM((width, channels), low),
            pltpu.VMEM((width, channels), low),
            pltpu.VMEM((width, channels), low),
            pltpu.VMEM((width, units), low),
            pltpu.VMEM((width, units), low),
            pltpu.VMEM((channels, channels), low),
            pltpu.VMEM((channels, channels), low),
            pltpu.VMEM((rows, width), low),
            pltpu.VMEM((rows, channels), high),
            pltpu.VMEM((MIX_GROUPS, 2, 2, own_rows, span), low),
            pltpu.VMEM((MIX_GROUPS, 2, own_rows, span), low),
            pltpu.VMEM((MIX_GROUPS, own_rows, span), low),
            pltpu.VMEM((MIX_GROUPS, own_rows, span), low),
            pltpu.VMEM((own_rows, width), low),
            pltpu.VMEM((2, n_tp, own_rows, width), low),
            pltpu.VMEM((2, rows, units), low),
            pltpu.VMEM((DOWN_GROUPS + 1, 2, 2, 2, own_rows, narrow), low),
            pltpu.VMEM((DOWN_GROUPS + 1, 2, 2, own_rows, narrow), low),
            pltpu.VMEM((DOWN_GROUPS + 1, 3, own_rows, narrow), low),
            pltpu.VMEM((DOWN_GROUPS + 1, 3, own_rows, narrow), low),
            pltpu.VMEM((16 * 1024, width // 8), low),
            pltpu.SemaphoreType.DMA((4,)),
            pltpu.SemaphoreType.DMA((7, n_fs // Y_SIZE)),
            pltpu.SemaphoreType.DMA((4,)),
            pltpu.SemaphoreType.DMA((3, n_fs // Y_SIZE)),
            pltpu.SemaphoreType.DMA((2 * MIX_GROUPS,)),
            pltpu.SemaphoreType.DMA((7,)),
            pltpu.SemaphoreType.DMA((DOWN_GROUPS + 1, 4)),
            pltpu.SemaphoreType.DMA((9,)),
        ],
        compiler_params=pltpu.CompilerParams(
            collective_id=0, has_side_effects=True, vmem_limit_bytes=60 * 1024 * 1024
        ),
        name="fused_layer",
    )(
        tokens,
        first_norm_scale.reshape(1, width),
        recurrent_branch_matrix,
        gelu_gate_matrix,
        filter_taps_weight,
        recurrence_gate_blocks,
        input_gate_blocks,
        base_decay_logits.reshape(1, channels),
        extra_log_decay,
        mixer_output_matrix,
        second_norm_scale.reshape(1, width),
        mixer_up_matrix,
        mixer_down_matrix,
    )


def solution(mesh):
    in_specs = (
        P("fs", None),
        P(),
        P("fs", "tp"),
        P("fs", "tp"),
        P(None, "tp"),
        P("tp", None, None),
        P("tp", None, None),
        P("tp"),
        P("fs", "tp"),
        P("fs", "tp"),
        P(),
        P("fs", "tp"),
        P("fs", "tp"),
    )
    out_specs = P(("fs", "tp"), None)
    body = functools.partial(fused_local, mesh) if fits(mesh) else local
    return jax.shard_map(body, mesh=mesh, in_specs=in_specs, out_specs=out_specs, check_vma=False)
```

```python
import functools

import jax
import jax.numpy as jnp
from jax import lax
from jax.experimental import pallas as pl
from jax.experimental.pallas import tpu as pltpu
from jax.sharding import PartitionSpec as P

epsilon = 1e-06
decay_rate_scale = 8.0


def rms_scaled(sequence_token_rows, scales):
    widened = sequence_token_rows.astype(jnp.float32)
    mean_square = jnp.mean(widened * widened, axis=-1, keepdims=True)
    return (widened * lax.rsqrt(mean_square + epsilon) * scales).astype(jnp.bfloat16)


def linear_combine(earlier, later):
    return (earlier[0] * later[0], later[0] * earlier[1] + later[1])


def causal_taps(branch, filter_taps_weight):
    tap_count = filter_taps_weight.shape[0]
    positions = branch.shape[0]
    padded = jnp.pad(branch.astype(jnp.float32), ((tap_count - 1, 0), (0, 0)))
    running = jnp.zeros(branch.shape, jnp.float32)
    for offset in range(tap_count):
        running = running + padded[offset : offset + positions] * filter_taps_weight[offset].astype(
            jnp.float32
        )
    return running.astype(jnp.bfloat16)


def block_map(convolved, blocks):
    positions, channels = convolved.shape
    grouped = convolved.reshape(positions, blocks.shape[0], blocks.shape[1])
    mapped = jnp.einsum("sgi,gij->sgj", grouped, blocks, preferred_element_type=jnp.float32)
    return jax.nn.sigmoid(mapped.reshape(positions, channels))


def contract_columns(left, right):
    return lax.dot_general(
        left, right, (((1,), (1,)), ((), ())), preferred_element_type=jnp.float32
    )


def local(
    tokens,
    first_norm_scale,
    recurrent_branch_matrix,
    gelu_gate_matrix,
    filter_taps_weight,
    recurrence_gate_blocks,
    input_gate_blocks,
    base_decay_logits,
    extra_log_decay,
    mixer_output_matrix,
    second_norm_scale,
    mixer_up_matrix,
    mixer_down_matrix,
):
    positions = tokens.shape[0]
    own_count = positions // lax.axis_size("tp")
    normed = rms_scaled(tokens, first_norm_scale)
    branch_sum = jnp.dot(
        normed,
        lax.all_gather(recurrent_branch_matrix, "fs", axis=0, tiled=True),
        preferred_element_type=jnp.float32,
    )
    gate_sum = jnp.dot(
        normed,
        lax.all_gather(gelu_gate_matrix, "fs", axis=0, tiled=True),
        preferred_element_type=jnp.float32,
    )
    branch = branch_sum.astype(jnp.bfloat16)
    gate_branch = gate_sum.astype(jnp.bfloat16)
    out_full = lax.all_gather(mixer_output_matrix, "fs", axis=0, tiled=True)
    convolved = causal_taps(branch, filter_taps_weight)
    recurrence_gate_value = block_map(convolved, recurrence_gate_blocks)
    admission = block_map(convolved, input_gate_blocks)
    log_keep_factor = (
        decay_rate_scale * recurrence_gate_value * jax.nn.log_sigmoid(base_decay_logits)
        + extra_log_decay
    )
    retain = jnp.exp(log_keep_factor)
    driven = jnp.sqrt(-jnp.expm1(2.0 * log_keep_factor)) * (
        admission * convolved.astype(jnp.float32)
    )
    memory = lax.associative_scan(linear_combine, (retain, driven), axis=0)[1]
    recurrent = (memory * jax.nn.gelu(gate_branch.astype(jnp.float32))).astype(jnp.bfloat16)
    up_full = lax.all_gather(mixer_up_matrix, "fs", axis=0, tiled=True)
    whole_sum = lax.psum(contract_columns(recurrent, out_full).astype(jnp.bfloat16), "tp").astype(
        jnp.float32
    )
    residual_all = (tokens.astype(jnp.float32) + whole_sum).astype(jnp.bfloat16)
    raised = jnp.dot(
        rms_scaled(residual_all, second_norm_scale), up_full, preferred_element_type=jnp.float32
    )
    hidden = jnp.square(jax.nn.relu(raised)).astype(jnp.bfloat16)
    residual = lax.dynamic_slice_in_dim(
        residual_all, lax.axis_index("tp") * own_count, own_count, 0
    )
    down_full = lax.all_gather(mixer_down_matrix, "fs", axis=0, tiled=True)
    channel_sum = lax.psum_scatter(
        contract_columns(hidden, down_full).astype(jnp.bfloat16),
        "tp",
        scatter_dimension=0,
        tiled=True,
    ).astype(jnp.float32)
    return (residual.astype(jnp.float32) + channel_sum).astype(jnp.bfloat16)


MESH = pl.DeviceIdType.MESH
Y_SIZE = 2
MIX_GROUPS = 4
DOWN_GROUPS = 8
STEPPED = (0, 1, 2, 3)
X_FIRST = (0, 2)


def fits(mesh):
    n_fs, n_tp = mesh.shape["fs"], mesh.shape["tp"]
    return n_tp == 2 * Y_SIZE and n_fs == 4 * Y_SIZE


def shifted_down(values, by, fill):
    if by % 8 == 0:
        top = jnp.full((by, values.shape[1]), fill, values.dtype)
        return jnp.concatenate([top, values[: values.shape[0] - by]], axis=0)
    rows = lax.broadcasted_iota(jnp.int32, values.shape, 0)
    return jnp.where(rows < by, fill, pltpu.roll(values, by, 0))


def one_minus_exp(exponent):
    series = 1.0
    for order in range(8, 1, -1):
        series = 1.0 + exponent * (1.0 / order) * series
    return jnp.where(exponent > -0.35, -exponent * series, 1.0 - jnp.exp(exponent))


def fused(
    nz,
    tok_in, scale1_in, wb, wg, taps_in, rblk_in, iblk_in, logits_in, extra_in, wo, scale2_in, wu, wd,
    result,
    scale1, taps, rblk, iblk, logits, scale2,
    normed, fb, fg, fo, fu, fd, rdiag, idiag, tok, extra,
    part1, pair1, give1, got1, res, mid, hidden,
    part2, pair2, give2, got2, tally,
    s_sem, along, lump, across, r_recv, a_recv, b_recv, l_sem,
):
    f = lax.axis_index("fs")
    t = lax.axis_index("tp")
    z, y = f // Y_SIZE, f % Y_SIZE
    x, c = t // 2, t % 2
    last = nz - 1
    parity = z % 2
    at_end = (z == 0) | (z == last)
    zmate = z + 1 - 2 * parity
    ymate = z * Y_SIZE + (1 - y)
    xmate = (1 - x) * 2 + c
    cmate = x * 2 + (1 - c)
    diagonal = (1 - x) * 2 + (1 - c)
    rows, width = tok.shape
    own_rows = result.shape[0]
    depth = wb.shape[0]
    half = depth // 2
    units = fu.shape[1]

    barrier = pltpu.get_barrier_semaphore()

    def greet(sem, device):
        pl.semaphore_signal(sem, inc=1, device_id=device, device_id_type=MESH)

    to_x = {"fs": f, "tp": xmate}
    to_c = {"fs": f, "tp": cmate}
    to_z = {"fs": zmate * Y_SIZE + y, "tp": t}
    to_d = {"fs": zmate * Y_SIZE + y, "tp": xmate}
    inside = jnp.logical_not(at_end)
    for k in range(1, nz):
        greet(barrier, {"fs": lax.rem(z + k, nz) * Y_SIZE + y, "tp": t})
    for device in ({"fs": ymate, "tp": t}, to_x, to_c, to_d):
        greet(barrier, device)
    early = [
        pltpu.make_async_copy(given, kept, l_sem.at[1 + i])
        for i, (given, kept) in enumerate(
            (
                (tok_in, tok),
                (scale1_in, scale1),
                (rblk_in, rblk),
                (iblk_in, iblk),
                (taps_in, taps),
                (logits_in, logits),
                (extra_in, extra),
                (scale2_in, scale2),
            )
        )
    ]

    for copy in early:
        copy.start()
    pl.semaphore_wait(barrier, nz + 3)

    def start(pred, copy):
        if pred is None:
            copy.start()
        else:
            pl.when(pred)(copy.start)

    def settle(count, sem):
        lot = tally.at[pl.ds(0, count * 16), :]
        pltpu.make_async_copy(lot, lot, sem).wait()

    plain = (wb, wg, wo)
    whole = (fb, fg, fo)
    lumped, single = (0, 1, 3, 4), (2, 5, 6)

    def source(g, way_parity):
        if g < 3:
            return plain[g]
        w = wu if g < 5 else wd
        first = half * ((g - 3) % 2)
        return w.at[
            pl.ds(first, half), pl.ds(pl.multiple_of(way_parity * units, units), units)
        ]

    def slot(g, zs, ys):
        if g < 3:
            return whole[g].at[pl.ds(pl.multiple_of((zs * Y_SIZE + ys) * depth, depth), depth), :]
        if g < 5:
            at = (zs * Y_SIZE + ys) * depth + (g - 3) * half
            return fu.at[pl.ds(pl.multiple_of(at, half), half), :]
        at = ((zs * 2 + (g - 5)) * Y_SIZE + ys) * half
        return fd.at[pl.ds(pl.multiple_of(at, half), half), :]

    def over(g, zs):
        return lump.at[lumped.index(g)] if g in lumped else across.at[single.index(g), zs]

    def z_copy(g, src, zs, zt):
        return pltpu.make_async_remote_copy(
            src_ref=src,
            dst_ref=slot(g, zs, y),
            send_sem=s_sem.at[0 if g < 3 else 1],
            recv_sem=along.at[g, zs],
            device_id={"fs": zt * Y_SIZE + y, "tp": t},
            device_id_type=MESH,
        )

    def y_copy(g, src, zs):
        return pltpu.make_async_remote_copy(
            src_ref=src,
            dst_ref=slot(g, zs, y),
            send_sem=s_sem.at[2],
            recv_sem=over(g, zs),
            device_id={"fs": ymate, "tp": t},
            device_id_type=MESH,
        )

    def landed(here, sem):
        pltpu.make_async_copy(here, here, sem).wait()

    def take(g, zs):
        landed(slot(g, zs, y), along.at[g, zs])

    def spread_z(g, outer=None, far=range(1, nz), held=None):
        for d in (1,) if g < 3 else far:
            for way in (0, 1):
                zt = z + d if way == 0 else z - d
                exists = zt <= last if way == 0 else zt >= 0
                if outer is not None:
                    to_end = (zt == 0) | (zt == last)
                    exists = exists & (to_end if outer else jnp.logical_not(to_end))
                if held is not None:
                    exists = exists & (at_end if held else jnp.logical_not(at_end))
                start(exists, z_copy(g, source(g, lax.rem(zt + nz, 2)), z, zt))

    def own(g, pred=None):
        start(pred, y_copy(g, source(g, parity), z))

    def forward(g, d):
        for way in (0, 1):
            zs = z - d if way == 0 else z + d
            exists = zs >= 0 if way == 0 else zs <= last
            pl.when(exists)(functools.partial(take, g, zs))
            if d < last:
                onward = z < last if way == 0 else z > 0
                zt = z + 1 if way == 0 else z - 1
                start(exists & onward, z_copy(g, slot(g, zs, y), zs, zt))
            start(exists, y_copy(g, slot(g, zs, y), zs))

    side = z // (nz // 2)
    origins = [zmate] + [rank + side * (last - 2 * rank) for rank in range(2, nz)]

    def hand_over(g, k, pred=None):
        if pred is None:
            take(g, origins[k])
        else:
            pl.when(pred)(functools.partial(take, g, origins[k]))
        start(pred, y_copy(g, slot(g, origins[k], y), origins[k]))

    def take_lump(g):
        count = nz * depth if g < 3 else nz * half
        landed((whole[g] if g < 3 else fu).at[pl.ds(0, count), :], over(g, 0))

    def take_over(g, zs):
        landed(slot(g, zs, 1 - y), over(g, zs))

    def near_copy(src, dst, device, sem):
        copy = pltpu.make_async_remote_copy(
            src_ref=src,
            dst_ref=dst,
            send_sem=s_sem.at[3],
            recv_sem=sem,
            device_id=device,
            device_id_type=MESH,
        )
        copy.start()
        return copy

    spread_z(0)
    own(0)
    spread_z(1)
    own(1)

    stays = [
        pltpu.make_async_copy(source(g, parity), slot(g, z, y), l_sem.at[0]) for g in range(7)
    ]
    for copy in stays:
        copy.start()
    for copy in early:
        copy.wait()
    block = rblk.shape[1]
    for blocks, diag in ((rblk, rdiag), (iblk, idiag)):
        diag[...] = jnp.zeros_like(diag)
        for b in range(rblk.shape[0]):
            diag[b * block : (b + 1) * block, b * block : (b + 1) * block] = blocks[b]

    def norm_rows(i, carry):
        at = pl.ds(pl.multiple_of(i * 32, 32), 32)
        normed[at, :] = rms_scaled(tok[at, :], scale1[...])
        return carry

    lax.fori_loop(0, rows // 32, norm_rows, 0)

    forward(0, 1)
    forward(1, 1)
    forward(0, 2)
    own(2)
    forward(1, 2)
    spread_z(2)
    forward(0, 3)
    forward(1, 3)
    forward(2, 1)
    spread_z(3, False)
    spread_z(4, False)
    settle(depth // 16 * 7, l_sem.at[0])
    take_lump(0)

    branch = jnp.dot(normed[...], fb[...], preferred_element_type=jnp.float32)
    branch = branch.astype(jnp.bfloat16).astype(jnp.float32)
    tap_count = taps.shape[0]
    running = branch * taps[tap_count - 1 : tap_count, :].astype(jnp.float32)
    for offset in range(tap_count - 1):
        by = tap_count - 1 - offset
        running = running + shifted_down(branch, by, 0.0) * taps[offset : offset + 1, :].astype(
            jnp.float32
        )
    convolved = running.astype(jnp.bfloat16)
    rate = jax.nn.sigmoid(jnp.dot(convolved, rdiag[...], preferred_element_type=jnp.float32))
    admission = jax.nn.sigmoid(jnp.dot(convolved, idiag[...], preferred_element_type=jnp.float32))
    base = -jnp.log1p(jnp.exp(-logits[...]))
    log_keep = decay_rate_scale * rate * base + extra[...]
    keep = jnp.exp(log_keep)
    memory = jnp.sqrt(one_minus_exp(2.0 * log_keep)) * (admission * convolved.astype(jnp.float32))
    by = 1
    while by < rows:
        memory = keep * shifted_down(memory, by, 0.0) + memory
        if 2 * by < rows:
            keep = keep * shifted_down(keep, by, 1.0)
        by *= 2
    forward(2, 2)
    take_lump(1)
    gate = jnp.dot(normed[...], fg[...], preferred_element_type=jnp.float32)
    gate = gate.astype(jnp.bfloat16).astype(jnp.float32)
    recurrent = (memory * jax.nn.gelu(gate)).astype(jnp.bfloat16)

    forward(2, 3)
    spread_z(3, True)
    spread_z(4, True)
    spread_z(5, False, held=False)
    spread_z(6, False, held=False)
    own(3)
    own(4)
    own(5, at_end)
    hand_over(3, 1, inside)
    hand_over(4, 1, inside)

    inner = z + side * (last - 2 * z)
    ranks = [inner, 1 - inner] + list(range(2, nz))
    order = [rank + side * (last - 2 * rank) for rank in ranks]
    span = width // MIX_GROUPS
    own_at = pl.ds(pl.multiple_of(t * own_rows, own_rows), own_rows)
    firsts, seconds = [], []

    def mix_columns(j):
        return pl.ds(pl.multiple_of(order[j] * span, span), span)

    def mix_first(j):
        firsts[j].wait_recv()
        away = part1[j, 1 - x, c].astype(jnp.float32) + pair1[j, 1 - x].astype(jnp.float32)
        give1[j] = away.astype(jnp.bfloat16)
        seconds.append(
            near_copy(give1.at[j], got1.at[j], to_x, r_recv.at[MIX_GROUPS + j])
        )

    def mix_second(j):
        seconds[j].wait_recv()
        mixed = part1[j, x, c].astype(jnp.float32) + pair1[j, x].astype(jnp.float32)
        mixed = mixed + got1[j].astype(jnp.float32)
        at = mix_columns(j)
        res[:, at] = (tok[own_at, at].astype(jnp.float32) + mixed).astype(jnp.bfloat16)

    for j in range(MIX_GROUPS):
        if j == 2:
            mix_first(1)
        take_over(2, order[j])
        product = contract_columns(recurrent, fo[mix_columns(j), :])
        part1[j] = product.astype(jnp.bfloat16).reshape(2, 2, own_rows, span)
        firsts.append(
            near_copy(part1.at[j, :, 1 - c], pair1.at[j], to_c, r_recv.at[j])
        )
        if j == 1:
            mix_first(0)
        if j > 1:
            mix_first(j)
    for j in range(MIX_GROUPS):
        mix_second(j)

    mid[parity, t] = rms_scaled(res[...], scale2[...])
    mine = mid.at[parity, t]
    theirs = mid.at[1 - parity, t]
    near_copy(mine, mine, to_x, a_recv.at[1])
    near_copy(mine, mine, to_z, a_recv.at[0])
    near_copy(mine, mine, to_c, a_recv.at[2])
    spread_z(5, False, held=True)
    spread_z(6, False, held=True)
    spread_z(5, True, (1,))
    spread_z(6, True, (1,))

    def arrived(here, index):
        landed(here, a_recv.at[index])

    def pass_on(here, device, index):
        near_copy(here, here, device, a_recv.at[index])

    beside = mid.at[parity, xmate]
    askew = mid.at[1 - parity, xmate]
    for g in (3, 4):
        for k in range(nz - 1):
            hand_over(g, k, at_end if k == 1 else None)
    own(5, inside)
    own(6)
    arrived(beside, 1)
    pass_on(beside, to_c, 5)
    arrived(theirs, 0)
    pass_on(theirs, to_x, 3)
    pass_on(theirs, to_c, 4)
    spread_z(5, True, range(2, nz))
    spread_z(6, True, range(2, nz))
    arrived(mid.at[parity, cmate], 2)
    arrived(mid.at[parity, diagonal], 5)
    take_lump(3)
    take_lump(4)

    tile = 256

    def up(par):
        def up_tile(i, carry):
            at = pl.ds(pl.multiple_of(i * tile, tile), tile)
            raised = jnp.dot(
                mid[par].reshape(rows, width), fu[:, at], preferred_element_type=jnp.float32
            )
            hidden[par, :, at] = jnp.square(jnp.maximum(raised, 0.0)).astype(jnp.bfloat16)
            return carry

        lax.fori_loop(0, units // tile, up_tile, 0)

    up(parity)
    hand_over(5, 0)
    arrived(askew, 3)
    pass_on(askew, to_c, 6)
    arrived(mid.at[1 - parity, cmate], 4)
    arrived(mid.at[1 - parity, diagonal], 6)
    up(1 - parity)

    narrow = width // DOWN_GROUPS
    halves = [k for r in range(2) for k in range(2)] + [k for k in range(2) for r in range(2, nz)]
    final = DOWN_GROUPS - 1
    lots = [(j, None) for j in range(final - 1)] + [(final, 0), (final - 1, None), (final, 1)]
    shared, spread = {}, {}
    level = jnp.where(at_end, 0, 1)

    def number(lot):
        j, which = lot
        if j >= 4:
            return j + (which or 0)
        return (level if j < 2 else 1 - level) * 2 + j % 2

    def place(j):
        if j < 4:
            return z if j < 2 else zmate
        rank = 2 + (j - 4) % (nz - 2)
        return rank + side * (last - 2 * rank)

    def signal_at(lot, k):
        return b_recv.at[number(lot), k]

    def lot_columns(lot):
        which = lot[1]
        return pl.ds(0, narrow if which is None else half)

    def lot_sides(lot):
        which = lot[1]
        return list(range(Y_SIZE)) if which is None else [y if which == 0 else 1 - y]

    def pair_sum(lot, par, xs):
        at = lot_columns(lot)
        mine = part2[number(lot), par, xs, c, :, at].astype(jnp.float32)
        return mine + pair2[number(lot), par, xs, :, at].astype(jnp.float32)

    def multiply(i):
        lot = lots[i]
        j, which = lot
        q = place(j)
        if which != 0:
            take_over(5 + halves[j], q)
        first = (q * 2 + halves[j]) * narrow
        if which is not None:
            first = first + lot_sides(lot)[0] * half
        at = lot_columns(lot)
        some = fd[pl.ds(pl.multiple_of(first, half), at.size), :]
        product = contract_columns(hidden[...].reshape(2 * rows, units), some)
        n = number(lot)
        part2[n, :, :, :, :, at] = product.astype(jnp.bfloat16).reshape(2, 2, 2, own_rows, at.size)
        shared[lot] = near_copy(
            part2.at[n, :, :, 1 - c, :, at], pair2.at[n, :, :, :, at], to_c, signal_at(lot, 0)
        )

    def exchange(i):
        lot = lots[i]
        shared[lot].wait_recv()
        at = lot_columns(lot)
        n = number(lot)
        if i in STEPPED:
            for k in range(2):
                away = pair_sum(lot, k, 1 - x) if i in X_FIRST else pair_sum(lot, 1 - parity, k)
                give2[n, k] = away.astype(jnp.bfloat16)
            two = pl.ds(0, 2)
            device = to_x if i in X_FIRST else to_z
            spread[lot] = [
                near_copy(give2.at[n, two], got2.at[n, two], device, signal_at(lot, 1))
            ]
            return
        ways = [
            (to_d, 1 - parity, 1 - x),
            (to_x, parity, 1 - x),
            (to_z, 1 - parity, x),
        ]
        spread[lot] = []
        for k, (device, par, xs) in enumerate(ways):
            give2[n, k, :, at] = pair_sum(lot, par, xs).astype(jnp.bfloat16)
            spread[lot].append(
                near_copy(
                    give2.at[n, k, :, at], got2.at[n, k, :, at], device, signal_at(lot, k + 1)
                )
            )

    def pass_across(i):
        lot = lots[i]
        spread[lot][0].wait_recv()
        n = number(lot)
        if i in X_FIRST:
            away = pair_sum(lot, 1 - parity, x) + got2[n, 1 - parity].astype(jnp.float32)
        else:
            away = pair_sum(lot, parity, 1 - x) + got2[n, 1 - x].astype(jnp.float32)
        give2[n, 2] = away.astype(jnp.bfloat16)
        device = to_z if i in X_FIRST else to_x
        spread[lot] = [near_copy(give2.at[n, 2], got2.at[n, 2], device, signal_at(lot, 2))]

    def finish(i):
        lot = lots[i]
        for copy in spread[lot]:
            copy.wait_recv()
        total = pair_sum(lot, parity, x)
        for k in [parity if i in X_FIRST else x, 2] if i in STEPPED else range(3):
            total = total + got2[number(lot), k, :, lot_columns(lot)].astype(jnp.float32)
        for k, ys in enumerate(lot_sides(lot)):
            first = (place(lot[0]) * Y_SIZE + ys) * depth + halves[lot[0]] * half
            at = pl.ds(pl.multiple_of(first, half), half)
            result[:, at] = (
                res[:, at].astype(jnp.float32) + total[:, k * half : (k + 1) * half]
            ).astype(jnp.bfloat16)

    plan = [
        (hand_over, 6, 0),
        (multiply, 0),
        (multiply, 1),
        (exchange, 0),
        (exchange, 1),
        (multiply, 2),
        (hand_over, 5, 1),
        (exchange, 2),
        (hand_over, 5, 2),
        (multiply, 3),
        (exchange, 3),
        (hand_over, 6, 1),
        (multiply, 4),
        (pass_across, 0),
        (exchange, 4),
        (hand_over, 6, 2),
        (multiply, 5),
        (pass_across, 1),
        (exchange, 5),
        (multiply, 6),
        (exchange, 6),
        (pass_across, 2),
        (multiply, 7),
        (exchange, 7),
        (pass_across, 3),
        (multiply, 8),
        (exchange, 8),
        (finish, 0),
        (finish, 1),
        (finish, 2),
        (finish, 3),
        (finish, 4),
        (finish, 5),
        (finish, 6),
        (finish, 7),
        (finish, 8),
    ]
    for step, *which in plan:
        step(*which)
    pl.when(at_end)(functools.partial(settle, depth // 16 * 3, s_sem.at[0]))
    relayed = 3 * (2 + nz - 1)
    pl.when(inside)(functools.partial(settle, depth // 16 * relayed, s_sem.at[0]))
    settle(depth // 16 * 4 * (nz - 1), s_sem.at[1])
    settle(depth // 16 * 7 * nz, s_sem.at[2])
    bits = own_rows * width // (16 * depth)
    mixed = own_rows * span // (16 * depth)
    summed = own_rows * narrow // (16 * depth)
    settle(7 * bits + 3 * MIX_GROUPS * mixed + 7 * DOWN_GROUPS * summed, s_sem.at[3])


def fused_local(
    mesh,
    tokens,
    first_norm_scale,
    recurrent_branch_matrix,
    gelu_gate_matrix,
    filter_taps_weight,
    recurrence_gate_blocks,
    input_gate_blocks,
    base_decay_logits,
    extra_log_decay,
    mixer_output_matrix,
    second_norm_scale,
    mixer_up_matrix,
    mixer_down_matrix,
):
    n_fs, n_tp = mesh.shape["fs"], mesh.shape["tp"]
    rows, width = tokens.shape
    own_rows = rows // n_tp
    channels = recurrent_branch_matrix.shape[1]
    units = mixer_up_matrix.shape[1] // 2
    span = width // MIX_GROUPS
    narrow = width // DOWN_GROUPS
    low, high = jnp.bfloat16, jnp.float32
    hbm = pl.BlockSpec(memory_space=pl.ANY)
    return pl.pallas_call(
        functools.partial(fused, n_fs // Y_SIZE),
        out_shape=pltpu.VMEM((own_rows, width), low),
        in_specs=[hbm] * 13,
        out_specs=pl.BlockSpec(memory_space=pltpu.VMEM),
        scratch_shapes=[
            pltpu.VMEM((1, width), high),
            pltpu.VMEM(filter_taps_weight.shape, low),
            pltpu.VMEM(recurrence_gate_blocks.shape, low),
            pltpu.VMEM(input_gate_blocks.shape, low),
            pltpu.VMEM((1, channels), high),
            pltpu.VMEM((1, width), high),
            pltpu.VMEM((rows, width), low),
            pltpu.VMEM((width, channels), low),
            pltpu.VMEM((width, channels), low),
            pltpu.VMEM((width, channels), low),
            pltpu.VMEM((width, units), low),
            pltpu.VMEM((width, units), low),
            pltpu.VMEM((channels, channels), low),
            pltpu.VMEM((channels, channels), low),
            pltpu.VMEM((rows, width), low),
            pltpu.VMEM((rows, channels), high),
            pltpu.VMEM((MIX_GROUPS, 2, 2, own_rows, span), low),
            pltpu.VMEM((MIX_GROUPS, 2, own_rows, span), low),
            pltpu.VMEM((MIX_GROUPS, own_rows, span), low),
            pltpu.VMEM((MIX_GROUPS, own_rows, span), low),
            pltpu.VMEM((own_rows, width), low),
            pltpu.VMEM((2, n_tp, own_rows, width), low),
            pltpu.VMEM((2, rows, units), low),
            pltpu.VMEM((DOWN_GROUPS + 1, 2, 2, 2, own_rows, narrow), low),
            pltpu.VMEM((DOWN_GROUPS + 1, 2, 2, own_rows, narrow), low),
            pltpu.VMEM((DOWN_GROUPS + 1, 3, own_rows, narrow), low),
            pltpu.VMEM((DOWN_GROUPS + 1, 3, own_rows, narrow), low),
            pltpu.VMEM((16 * 1024, width // 8), low),
            pltpu.SemaphoreType.DMA((4,)),
            pltpu.SemaphoreType.DMA((7, n_fs // Y_SIZE)),
            pltpu.SemaphoreType.DMA((4,)),
            pltpu.SemaphoreType.DMA((3, n_fs // Y_SIZE)),
            pltpu.SemaphoreType.DMA((2 * MIX_GROUPS,)),
            pltpu.SemaphoreType.DMA((7,)),
            pltpu.SemaphoreType.DMA((DOWN_GROUPS + 1, 4)),
            pltpu.SemaphoreType.DMA((9,)),
        ],
        compiler_params=pltpu.CompilerParams(
            collective_id=0, has_side_effects=True, vmem_limit_bytes=60 * 1024 * 1024
        ),
        name="fused_layer",
    )(
        tokens,
        first_norm_scale.reshape(1, width),
        recurrent_branch_matrix,
        gelu_gate_matrix,
        filter_taps_weight,
        recurrence_gate_blocks,
        input_gate_blocks,
        base_decay_logits.reshape(1, channels),
        extra_log_decay,
        mixer_output_matrix,
        second_norm_scale.reshape(1, width),
        mixer_up_matrix,
        mixer_down_matrix,
    )


def solution(mesh):
    in_specs = (
        P("fs", None),
        P(),
        P("fs", "tp"),
        P("fs", "tp"),
        P(None, "tp"),
        P("tp", None, None),
        P("tp", None, None),
        P("tp"),
        P("fs", "tp"),
        P("fs", "tp"),
        P(),
        P("fs", "tp"),
        P("fs", "tp"),
    )
    out_specs = P(("fs", "tp"), None)
    body = functools.partial(fused_local, mesh) if fits(mesh) else local
    return jax.shard_map(body, mesh=mesh, in_specs=in_specs, out_specs=out_specs, check_vma=False)
```

```python
import functools

import jax
import jax.numpy as jnp
from jax import lax
from jax.experimental import pallas as pl
from jax.experimental.pallas import tpu as pltpu
from jax.sharding import PartitionSpec as P

epsilon = 1e-06
decay_rate_scale = 8.0


def rms_scaled(sequence_token_rows, scales):
    widened = sequence_token_rows.astype(jnp.float32)
    mean_square = jnp.mean(widened * widened, axis=-1, keepdims=True)
    return (widened * lax.rsqrt(mean_square + epsilon) * scales).astype(jnp.bfloat16)


def linear_combine(earlier, later):
    return (earlier[0] * later[0], later[0] * earlier[1] + later[1])


def causal_taps(branch, filter_taps_weight):
    tap_count = filter_taps_weight.shape[0]
    positions = branch.shape[0]
    padded = jnp.pad(branch.astype(jnp.float32), ((tap_count - 1, 0), (0, 0)))
    running = jnp.zeros(branch.shape, jnp.float32)
    for offset in range(tap_count):
        running = running + padded[offset : offset + positions] * filter_taps_weight[offset].astype(
            jnp.float32
        )
    return running.astype(jnp.bfloat16)


def block_map(convolved, blocks):
    positions, channels = convolved.shape
    grouped = convolved.reshape(positions, blocks.shape[0], blocks.shape[1])
    mapped = jnp.einsum("sgi,gij->sgj", grouped, blocks, preferred_element_type=jnp.float32)
    return jax.nn.sigmoid(mapped.reshape(positions, channels))


def contract_columns(left, right):
    return lax.dot_general(
        left, right, (((1,), (1,)), ((), ())), preferred_element_type=jnp.float32
    )


def local(
    tokens,
    first_norm_scale,
    recurrent_branch_matrix,
    gelu_gate_matrix,
    filter_taps_weight,
    recurrence_gate_blocks,
    input_gate_blocks,
    base_decay_logits,
    extra_log_decay,
    mixer_output_matrix,
    second_norm_scale,
    mixer_up_matrix,
    mixer_down_matrix,
):
    positions = tokens.shape[0]
    own_count = positions // lax.axis_size("tp")
    normed = rms_scaled(tokens, first_norm_scale)
    branch_sum = jnp.dot(
        normed,
        lax.all_gather(recurrent_branch_matrix, "fs", axis=0, tiled=True),
        preferred_element_type=jnp.float32,
    )
    gate_sum = jnp.dot(
        normed,
        lax.all_gather(gelu_gate_matrix, "fs", axis=0, tiled=True),
        preferred_element_type=jnp.float32,
    )
    branch = branch_sum.astype(jnp.bfloat16)
    gate_branch = gate_sum.astype(jnp.bfloat16)
    out_full = lax.all_gather(mixer_output_matrix, "fs", axis=0, tiled=True)
    convolved = causal_taps(branch, filter_taps_weight)
    recurrence_gate_value = block_map(convolved, recurrence_gate_blocks)
    admission = block_map(convolved, input_gate_blocks)
    log_keep_factor = (
        decay_rate_scale * recurrence_gate_value * jax.nn.log_sigmoid(base_decay_logits)
        + extra_log_decay
    )
    retain = jnp.exp(log_keep_factor)
    driven = jnp.sqrt(-jnp.expm1(2.0 * log_keep_factor)) * (
        admission * convolved.astype(jnp.float32)
    )
    memory = lax.associative_scan(linear_combine, (retain, driven), axis=0)[1]
    recurrent = (memory * jax.nn.gelu(gate_branch.astype(jnp.float32))).astype(jnp.bfloat16)
    up_full = lax.all_gather(mixer_up_matrix, "fs", axis=0, tiled=True)
    whole_sum = lax.psum(contract_columns(recurrent, out_full).astype(jnp.bfloat16), "tp").astype(
        jnp.float32
    )
    residual_all = (tokens.astype(jnp.float32) + whole_sum).astype(jnp.bfloat16)
    raised = jnp.dot(
        rms_scaled(residual_all, second_norm_scale), up_full, preferred_element_type=jnp.float32
    )
    hidden = jnp.square(jax.nn.relu(raised)).astype(jnp.bfloat16)
    residual = lax.dynamic_slice_in_dim(
        residual_all, lax.axis_index("tp") * own_count, own_count, 0
    )
    down_full = lax.all_gather(mixer_down_matrix, "fs", axis=0, tiled=True)
    channel_sum = lax.psum_scatter(
        contract_columns(hidden, down_full).astype(jnp.bfloat16),
        "tp",
        scatter_dimension=0,
        tiled=True,
    ).astype(jnp.float32)
    return (residual.astype(jnp.float32) + channel_sum).astype(jnp.bfloat16)


MESH = pl.DeviceIdType.MESH
Y_SIZE = 2
MIX_GROUPS = 4
DOWN_GROUPS = 8
STEPPED = (0, 2)
X_FIRST = (0, 2)


def fits(mesh):
    n_fs, n_tp = mesh.shape["fs"], mesh.shape["tp"]
    return n_tp == 2 * Y_SIZE and n_fs == 4 * Y_SIZE


def shifted_down(values, by, fill):
    if by % 8 == 0:
        top = jnp.full((by, values.shape[1]), fill, values.dtype)
        return jnp.concatenate([top, values[: values.shape[0] - by]], axis=0)
    rows = lax.broadcasted_iota(jnp.int32, values.shape, 0)
    return jnp.where(rows < by, fill, pltpu.roll(values, by, 0))


def one_minus_exp(exponent):
    series = 1.0
    for order in range(8, 1, -1):
        series = 1.0 + exponent * (1.0 / order) * series
    return jnp.where(exponent > -0.35, -exponent * series, 1.0 - jnp.exp(exponent))


def fused(
    nz,
    tok_in, scale1_in, wb, wg, taps_in, rblk_in, iblk_in, logits_in, extra_in, wo, scale2_in, wu, wd,
    result,
    scale1, taps, rblk, iblk, logits, scale2,
    normed, fb, fg, fo, fu, fd, rdiag, idiag, tok, extra,
    part1, pair1, give1, got1, res, mid, hidden,
    part2, pair2, give2, got2, tally,
    s_sem, along, lump, across, r_recv, a_recv, b_recv, l_sem,
):
    f = lax.axis_index("fs")
    t = lax.axis_index("tp")
    z, y = f // Y_SIZE, f % Y_SIZE
    x, c = t // 2, t % 2
    last = nz - 1
    parity = z % 2
    at_end = (z == 0) | (z == last)
    zmate = z + 1 - 2 * parity
    ymate = z * Y_SIZE + (1 - y)
    xmate = (1 - x) * 2 + c
    cmate = x * 2 + (1 - c)
    diagonal = (1 - x) * 2 + (1 - c)
    rows, width = tok.shape
    own_rows = result.shape[0]
    depth = wb.shape[0]
    half = depth // 2
    units = fu.shape[1]

    barrier = pltpu.get_barrier_semaphore()

    def greet(sem, device):
        pl.semaphore_signal(sem, inc=1, device_id=device, device_id_type=MESH)

    to_x = {"fs": f, "tp": xmate}
    to_c = {"fs": f, "tp": cmate}
    to_z = {"fs": zmate * Y_SIZE + y, "tp": t}
    to_d = {"fs": zmate * Y_SIZE + y, "tp": xmate}
    inside = jnp.logical_not(at_end)
    for k in range(1, nz):
        greet(barrier, {"fs": lax.rem(z + k, nz) * Y_SIZE + y, "tp": t})
    for device in ({"fs": ymate, "tp": t}, to_x, to_c, to_d):
        greet(barrier, device)
    early = [
        pltpu.make_async_copy(given, kept, l_sem.at[1 + i])
        for i, (given, kept) in enumerate(
            (
                (tok_in, tok),
                (scale1_in, scale1),
                (rblk_in, rblk),
                (iblk_in, iblk),
                (taps_in, taps),
                (logits_in, logits),
                (extra_in, extra),
                (scale2_in, scale2),
            )
        )
    ]

    for copy in early:
        copy.start()
    pl.semaphore_wait(barrier, nz + 3)

    def start(pred, copy):
        if pred is None:
            copy.start()
        else:
            pl.when(pred)(copy.start)

    def settle(count, sem):
        lot = tally.at[pl.ds(0, count * 16), :]
        pltpu.make_async_copy(lot, lot, sem).wait()

    plain = (wb, wg, wo)
    whole = (fb, fg, fo)
    lumped, single = (0, 1, 3, 4), (2, 5, 6)

    def source(g, way_parity):
        if g < 3:
            return plain[g]
        w = wu if g < 5 else wd
        first = half * ((g - 3) % 2)
        return w.at[
            pl.ds(first, half), pl.ds(pl.multiple_of(way_parity * units, units), units)
        ]

    def slot(g, zs, ys):
        if g < 3:
            return whole[g].at[pl.ds(pl.multiple_of((zs * Y_SIZE + ys) * depth, depth), depth), :]
        if g < 5:
            at = (zs * Y_SIZE + ys) * depth + (g - 3) * half
            return fu.at[pl.ds(pl.multiple_of(at, half), half), :]
        at = ((zs * 2 + (g - 5)) * Y_SIZE + ys) * half
        return fd.at[pl.ds(pl.multiple_of(at, half), half), :]

    def over(g, zs):
        return lump.at[lumped.index(g)] if g in lumped else across.at[single.index(g), zs]

    def z_copy(g, src, zs, zt):
        return pltpu.make_async_remote_copy(
            src_ref=src,
            dst_ref=slot(g, zs, y),
            send_sem=s_sem.at[0 if g < 3 else 1],
            recv_sem=along.at[g, zs],
            device_id={"fs": zt * Y_SIZE + y, "tp": t},
            device_id_type=MESH,
        )

    def y_copy(g, src, zs):
        return pltpu.make_async_remote_copy(
            src_ref=src,
            dst_ref=slot(g, zs, y),
            send_sem=s_sem.at[2],
            recv_sem=over(g, zs),
            device_id={"fs": ymate, "tp": t},
            device_id_type=MESH,
        )

    def landed(here, sem):
        pltpu.make_async_copy(here, here, sem).wait()

    def take(g, zs):
        landed(slot(g, zs, y), along.at[g, zs])

    def spread_z(g, outer=None, far=range(1, nz), held=None):
        for d in (1,) if g < 3 else far:
            for way in (0, 1):
                zt = z + d if way == 0 else z - d
                exists = zt <= last if way == 0 else zt >= 0
                if outer is not None:
                    to_end = (zt == 0) | (zt == last)
                    exists = exists & (to_end if outer else jnp.logical_not(to_end))
                if held is not None:
                    exists = exists & (at_end if held else jnp.logical_not(at_end))
                start(exists, z_copy(g, source(g, lax.rem(zt + nz, 2)), z, zt))

    def own(g, pred=None):
        start(pred, y_copy(g, source(g, parity), z))

    def forward(g, d):
        for way in (0, 1):
            zs = z - d if way == 0 else z + d
            exists = zs >= 0 if way == 0 else zs <= last
            pl.when(exists)(functools.partial(take, g, zs))
            if d < last:
                onward = z < last if way == 0 else z > 0
                zt = z + 1 if way == 0 else z - 1
                start(exists & onward, z_copy(g, slot(g, zs, y), zs, zt))
            start(exists, y_copy(g, slot(g, zs, y), zs))

    side = z // (nz // 2)
    origins = [zmate] + [rank + side * (last - 2 * rank) for rank in range(2, nz)]

    def hand_over(g, k, pred=None):
        if pred is None:
            take(g, origins[k])
        else:
            pl.when(pred)(functools.partial(take, g, origins[k]))
        start(pred, y_copy(g, slot(g, origins[k], y), origins[k]))

    def take_lump(g):
        count = nz * depth if g < 3 else nz * half
        landed((whole[g] if g < 3 else fu).at[pl.ds(0, count), :], over(g, 0))

    def take_over(g, zs):
        landed(slot(g, zs, 1 - y), over(g, zs))

    def near_copy(src, dst, device, sem):
        copy = pltpu.make_async_remote_copy(
            src_ref=src,
            dst_ref=dst,
            send_sem=s_sem.at[3],
            recv_sem=sem,
            device_id=device,
            device_id_type=MESH,
        )
        copy.start()
        return copy

    spread_z(0)
    own(0)
    spread_z(1)
    own(1)

    stays = [
        pltpu.make_async_copy(source(g, parity), slot(g, z, y), l_sem.at[0]) for g in range(7)
    ]
    for copy in stays:
        copy.start()
    for copy in early:
        copy.wait()
    block = rblk.shape[1]
    for blocks, diag in ((rblk, rdiag), (iblk, idiag)):
        diag[...] = jnp.zeros_like(diag)
        for b in range(rblk.shape[0]):
            diag[b * block : (b + 1) * block, b * block : (b + 1) * block] = blocks[b]

    def norm_rows(i, carry):
        at = pl.ds(pl.multiple_of(i * 32, 32), 32)
        normed[at, :] = rms_scaled(tok[at, :], scale1[...])
        return carry

    lax.fori_loop(0, rows // 32, norm_rows, 0)

    forward(0, 1)
    forward(1, 1)
    forward(0, 2)
    own(2)
    forward(1, 2)
    spread_z(2)
    forward(0, 3)
    forward(1, 3)
    forward(2, 1)
    spread_z(3, False)
    spread_z(4, False)
    settle(depth // 16 * 7, l_sem.at[0])
    take_lump(0)

    branch = jnp.dot(normed[...], fb[...], preferred_element_type=jnp.float32)
    branch = branch.astype(jnp.bfloat16).astype(jnp.float32)
    tap_count = taps.shape[0]
    running = branch * taps[tap_count - 1 : tap_count, :].astype(jnp.float32)
    for offset in range(tap_count - 1):
        by = tap_count - 1 - offset
        running = running + shifted_down(branch, by, 0.0) * taps[offset : offset + 1, :].astype(
            jnp.float32
        )
    convolved = running.astype(jnp.bfloat16)
    rate = jax.nn.sigmoid(jnp.dot(convolved, rdiag[...], preferred_element_type=jnp.float32))
    admission = jax.nn.sigmoid(jnp.dot(convolved, idiag[...], preferred_element_type=jnp.float32))
    base = -jnp.log1p(jnp.exp(-logits[...]))
    log_keep = decay_rate_scale * rate * base + extra[...]
    keep = jnp.exp(log_keep)
    memory = jnp.sqrt(one_minus_exp(2.0 * log_keep)) * (admission * convolved.astype(jnp.float32))
    by = 1
    while by < rows:
        memory = keep * shifted_down(memory, by, 0.0) + memory
        if 2 * by < rows:
            keep = keep * shifted_down(keep, by, 1.0)
        by *= 2
    forward(2, 2)
    take_lump(1)
    gate = jnp.dot(normed[...], fg[...], preferred_element_type=jnp.float32)
    gate = gate.astype(jnp.bfloat16).astype(jnp.float32)
    recurrent = (memory * jax.nn.gelu(gate)).astype(jnp.bfloat16)

    forward(2, 3)
    spread_z(3, True)
    spread_z(4, True)
    spread_z(5, False, held=False)
    spread_z(6, False, held=False)
    own(3)
    own(4)
    own(5, at_end)
    hand_over(3, 1, inside)
    hand_over(4, 1, inside)
    own(5, inside)

    inner = z + side * (last - 2 * z)
    ranks = [inner, 1 - inner] + list(range(2, nz))
    order = [rank + side * (last - 2 * rank) for rank in ranks]
    span = width // MIX_GROUPS
    own_at = pl.ds(pl.multiple_of(t * own_rows, own_rows), own_rows)
    firsts, seconds = [], []

    def mix_columns(j):
        return pl.ds(pl.multiple_of(order[j] * span, span), span)

    def mix_first(j):
        firsts[j].wait_recv()
        away = part1[j, 1 - x, c].astype(jnp.float32) + pair1[j, 1 - x].astype(jnp.float32)
        give1[j] = away.astype(jnp.bfloat16)
        seconds.append(
            near_copy(give1.at[j], got1.at[j], to_x, r_recv.at[MIX_GROUPS + j])
        )

    def mix_second(j):
        seconds[j].wait_recv()
        mixed = part1[j, x, c].astype(jnp.float32) + pair1[j, x].astype(jnp.float32)
        mixed = mixed + got1[j].astype(jnp.float32)
        at = mix_columns(j)
        res[:, at] = (tok[own_at, at].astype(jnp.float32) + mixed).astype(jnp.bfloat16)

    for j in range(MIX_GROUPS):
        if j == 2:
            mix_first(1)
        take_over(2, order[j])
        product = contract_columns(recurrent, fo[mix_columns(j), :])
        part1[j] = product.astype(jnp.bfloat16).reshape(2, 2, own_rows, span)
        firsts.append(
            near_copy(part1.at[j, :, 1 - c], pair1.at[j], to_c, r_recv.at[j])
        )
        if j == 1:
            mix_first(0)
        if j > 1:
            mix_first(j)
    for j in range(MIX_GROUPS):
        mix_second(j)

    mid[parity, t] = rms_scaled(res[...], scale2[...])
    mine = mid.at[parity, t]
    theirs = mid.at[1 - parity, t]
    near_copy(mine, mine, to_x, a_recv.at[1])
    near_copy(mine, mine, to_z, a_recv.at[0])
    near_copy(mine, mine, to_c, a_recv.at[2])
    spread_z(5, False, held=True)
    spread_z(6, False, held=True)
    spread_z(5, True, (1,))
    spread_z(6, True, (1,))

    def arrived(here, index):
        landed(here, a_recv.at[index])

    def pass_on(here, device, index):
        near_copy(here, here, device, a_recv.at[index])

    beside = mid.at[parity, xmate]
    askew = mid.at[1 - parity, xmate]
    for g in (3, 4):
        for k in range(nz - 1):
            hand_over(g, k, at_end if k == 1 else None)
    own(6)
    arrived(beside, 1)
    pass_on(beside, to_c, 5)
    arrived(theirs, 0)
    pass_on(theirs, to_x, 3)
    pass_on(theirs, to_c, 4)
    spread_z(5, True, range(2, nz))
    spread_z(6, True, range(2, nz))
    arrived(mid.at[parity, cmate], 2)
    arrived(mid.at[parity, diagonal], 5)
    take_lump(3)
    take_lump(4)

    tile = 256

    def up(par):
        def up_tile(i, carry):
            at = pl.ds(pl.multiple_of(i * tile, tile), tile)
            raised = jnp.dot(
                mid[par].reshape(rows, width), fu[:, at], preferred_element_type=jnp.float32
            )
            hidden[par, :, at] = jnp.square(jnp.maximum(raised, 0.0)).astype(jnp.bfloat16)
            return carry

        lax.fori_loop(0, units // tile, up_tile, 0)

    up(parity)
    hand_over(5, 0)
    arrived(askew, 3)
    pass_on(askew, to_c, 6)
    arrived(mid.at[1 - parity, cmate], 4)
    arrived(mid.at[1 - parity, diagonal], 6)
    up(1 - parity)

    narrow = width // DOWN_GROUPS
    halves = [k for r in range(2) for k in range(2)] + [k for k in range(2) for r in range(2, nz)]
    final = DOWN_GROUPS - 1
    lots = [(j, None) for j in range(final - 1)] + [(final, 0), (final - 1, None), (final, 1)]
    shared, spread = {}, {}
    level = jnp.where(at_end, 0, 1)

    def number(lot):
        j, which = lot
        if j >= 4:
            return j + (which or 0)
        return (level if j < 2 else 1 - level) * 2 + j % 2

    def place(j):
        if j < 4:
            return z if j < 2 else zmate
        rank = 2 + (j - 4) % (nz - 2)
        return rank + side * (last - 2 * rank)

    def signal_at(lot, k):
        return b_recv.at[number(lot), k]

    def lot_columns(lot):
        which = lot[1]
        return pl.ds(0, narrow if which is None else half)

    def lot_sides(lot):
        which = lot[1]
        return list(range(Y_SIZE)) if which is None else [y if which == 0 else 1 - y]

    def pair_sum(lot, par, xs):
        at = lot_columns(lot)
        mine = part2[number(lot), par, xs, c, :, at].astype(jnp.float32)
        return mine + pair2[number(lot), par, xs, :, at].astype(jnp.float32)

    def multiply(i):
        lot = lots[i]
        j, which = lot
        q = place(j)
        if which != 0:
            take_over(5 + halves[j], q)
        first = (q * 2 + halves[j]) * narrow
        if which is not None:
            first = first + lot_sides(lot)[0] * half
        at = lot_columns(lot)
        some = fd[pl.ds(pl.multiple_of(first, half), at.size), :]
        product = contract_columns(hidden[...].reshape(2 * rows, units), some)
        n = number(lot)
        part2[n, :, :, :, :, at] = product.astype(jnp.bfloat16).reshape(2, 2, 2, own_rows, at.size)
        shared[lot] = near_copy(
            part2.at[n, :, :, 1 - c, :, at], pair2.at[n, :, :, :, at], to_c, signal_at(lot, 0)
        )

    def exchange(i):
        lot = lots[i]
        shared[lot].wait_recv()
        at = lot_columns(lot)
        n = number(lot)
        if i in STEPPED:
            for k in range(2):
                away = pair_sum(lot, k, 1 - x) if i in X_FIRST else pair_sum(lot, 1 - parity, k)
                give2[n, k] = away.astype(jnp.bfloat16)
            two = pl.ds(0, 2)
            device = to_x if i in X_FIRST else to_z
            spread[lot] = [
                near_copy(give2.at[n, two], got2.at[n, two], device, signal_at(lot, 1))
            ]
            return
        ways = [
            (to_d, 1 - parity, 1 - x),
            (to_x, parity, 1 - x),
            (to_z, 1 - parity, x),
        ]
        spread[lot] = []
        for k, (device, par, xs) in enumerate(ways):
            give2[n, k, :, at] = pair_sum(lot, par, xs).astype(jnp.bfloat16)
            spread[lot].append(
                near_copy(
                    give2.at[n, k, :, at], got2.at[n, k, :, at], device, signal_at(lot, k + 1)
                )
            )

    def pass_across(i):
        lot = lots[i]
        spread[lot][0].wait_recv()
        n = number(lot)
        if i in X_FIRST:
            away = pair_sum(lot, 1 - parity, x) + got2[n, 1 - parity].astype(jnp.float32)
        else:
            away = pair_sum(lot, parity, 1 - x) + got2[n, 1 - x].astype(jnp.float32)
        give2[n, 2] = away.astype(jnp.bfloat16)
        device = to_z if i in X_FIRST else to_x
        spread[lot] = [near_copy(give2.at[n, 2], got2.at[n, 2], device, signal_at(lot, 2))]

    def finish(i):
        lot = lots[i]
        for copy in spread[lot]:
            copy.wait_recv()
        total = pair_sum(lot, parity, x)
        for k in [parity if i in X_FIRST else x, 2] if i in STEPPED else range(3):
            total = total + got2[number(lot), k, :, lot_columns(lot)].astype(jnp.float32)
        for k, ys in enumerate(lot_sides(lot)):
            first = (place(lot[0]) * Y_SIZE + ys) * depth + halves[lot[0]] * half
            at = pl.ds(pl.multiple_of(first, half), half)
            result[:, at] = (
                res[:, at].astype(jnp.float32) + total[:, k * half : (k + 1) * half]
            ).astype(jnp.bfloat16)

    plan = [
        (hand_over, 6, 0),
        (multiply, 0),
        (multiply, 1),
        (exchange, 0),
        (exchange, 1),
        (multiply, 2),
        (hand_over, 5, 1),
        (exchange, 2),
        (hand_over, 5, 2),
        (multiply, 3),
        (exchange, 3),
        (hand_over, 6, 1),
        (multiply, 4),
        (pass_across, 0),
        (exchange, 4),
        (hand_over, 6, 2),
        (multiply, 5),
        (exchange, 5),
        (pass_across, 2),
        (multiply, 6),
        (exchange, 6),
        (multiply, 7),
        (exchange, 7),
        (multiply, 8),
        (exchange, 8),
        (finish, 4),
        (finish, 5),
        (finish, 6),
        (finish, 0),
        (finish, 1),
        (finish, 2),
        (finish, 3),
        (finish, 7),
        (finish, 8),
    ]
    for step, *which in plan:
        step(*which)
    pl.when(at_end)(functools.partial(settle, depth // 16 * 3, s_sem.at[0]))
    relayed = 3 * (2 + nz - 1)
    pl.when(inside)(functools.partial(settle, depth // 16 * relayed, s_sem.at[0]))
    settle(depth // 16 * 4 * (nz - 1), s_sem.at[1])
    settle(depth // 16 * 7 * nz, s_sem.at[2])
    bits = own_rows * width // (16 * depth)
    mixed = own_rows * span // (16 * depth)
    summed = own_rows * narrow // (16 * depth)
    settle(7 * bits + 3 * MIX_GROUPS * mixed + 7 * DOWN_GROUPS * summed, s_sem.at[3])


def fused_local(
    mesh,
    tokens,
    first_norm_scale,
    recurrent_branch_matrix,
    gelu_gate_matrix,
    filter_taps_weight,
    recurrence_gate_blocks,
    input_gate_blocks,
    base_decay_logits,
    extra_log_decay,
    mixer_output_matrix,
    second_norm_scale,
    mixer_up_matrix,
    mixer_down_matrix,
):
    n_fs, n_tp = mesh.shape["fs"], mesh.shape["tp"]
    rows, width = tokens.shape
    own_rows = rows // n_tp
    channels = recurrent_branch_matrix.shape[1]
    units = mixer_up_matrix.shape[1] // 2
    span = width // MIX_GROUPS
    narrow = width // DOWN_GROUPS
    low, high = jnp.bfloat16, jnp.float32
    hbm = pl.BlockSpec(memory_space=pl.ANY)
    return pl.pallas_call(
        functools.partial(fused, n_fs // Y_SIZE),
        out_shape=pltpu.VMEM((own_rows, width), low),
        in_specs=[hbm] * 13,
        out_specs=pl.BlockSpec(memory_space=pltpu.VMEM),
        scratch_shapes=[
            pltpu.VMEM((1, width), high),
            pltpu.VMEM(filter_taps_weight.shape, low),
            pltpu.VMEM(recurrence_gate_blocks.shape, low),
            pltpu.VMEM(input_gate_blocks.shape, low),
            pltpu.VMEM((1, channels), high),
            pltpu.VMEM((1, width), high),
            pltpu.VMEM((rows, width), low),
            pltpu.VMEM((width, channels), low),
            pltpu.VMEM((width, channels), low),
            pltpu.VMEM((width, channels), low),
            pltpu.VMEM((width, units), low),
            pltpu.VMEM((width, units), low),
            pltpu.VMEM((channels, channels), low),
            pltpu.VMEM((channels, channels), low),
            pltpu.VMEM((rows, width), low),
            pltpu.VMEM((rows, channels), high),
            pltpu.VMEM((MIX_GROUPS, 2, 2, own_rows, span), low),
            pltpu.VMEM((MIX_GROUPS, 2, own_rows, span), low),
            pltpu.VMEM((MIX_GROUPS, own_rows, span), low),
            pltpu.VMEM((MIX_GROUPS, own_rows, span), low),
            pltpu.VMEM((own_rows, width), low),
            pltpu.VMEM((2, n_tp, own_rows, width), low),
            pltpu.VMEM((2, rows, units), low),
            pltpu.VMEM((DOWN_GROUPS + 1, 2, 2, 2, own_rows, narrow), low),
            pltpu.VMEM((DOWN_GROUPS + 1, 2, 2, own_rows, narrow), low),
            pltpu.VMEM((DOWN_GROUPS + 1, 3, own_rows, narrow), low),
            pltpu.VMEM((DOWN_GROUPS + 1, 3, own_rows, narrow), low),
            pltpu.VMEM((16 * 1024, width // 8), low),
            pltpu.SemaphoreType.DMA((4,)),
            pltpu.SemaphoreType.DMA((7, n_fs // Y_SIZE)),
            pltpu.SemaphoreType.DMA((4,)),
            pltpu.SemaphoreType.DMA((3, n_fs // Y_SIZE)),
            pltpu.SemaphoreType.DMA((2 * MIX_GROUPS,)),
            pltpu.SemaphoreType.DMA((7,)),
            pltpu.SemaphoreType.DMA((DOWN_GROUPS + 1, 4)),
            pltpu.SemaphoreType.DMA((9,)),
        ],
        compiler_params=pltpu.CompilerParams(
            collective_id=0, has_side_effects=True, vmem_limit_bytes=60 * 1024 * 1024
        ),
        name="fused_layer",
    )(
        tokens,
        first_norm_scale.reshape(1, width),
        recurrent_branch_matrix,
        gelu_gate_matrix,
        filter_taps_weight,
        recurrence_gate_blocks,
        input_gate_blocks,
        base_decay_logits.reshape(1, channels),
        extra_log_decay,
        mixer_output_matrix,
        second_norm_scale.reshape(1, width),
        mixer_up_matrix,
        mixer_down_matrix,
    )


def solution(mesh):
    in_specs = (
        P("fs", None),
        P(),
        P("fs", "tp"),
        P("fs", "tp"),
        P(None, "tp"),
        P("tp", None, None),
        P("tp", None, None),
        P("tp"),
        P("fs", "tp"),
        P("fs", "tp"),
        P(),
        P("fs", "tp"),
        P("fs", "tp"),
    )
    out_specs = P(("fs", "tp"), None)
    body = functools.partial(fused_local, mesh) if fits(mesh) else local
    return jax.shard_map(body, mesh=mesh, in_specs=in_specs, out_specs=out_specs, check_vma=False)
```

```python
import functools

import jax
import jax.numpy as jnp
from jax import lax
from jax.experimental import pallas as pl
from jax.experimental.pallas import tpu as pltpu
from jax.sharding import PartitionSpec as P

epsilon = 1e-06
decay_rate_scale = 8.0


def rms_scaled(sequence_token_rows, scales):
    widened = sequence_token_rows.astype(jnp.float32)
    mean_square = jnp.mean(widened * widened, axis=-1, keepdims=True)
    return (widened * lax.rsqrt(mean_square + epsilon) * scales).astype(jnp.bfloat16)


def linear_combine(earlier, later):
    return (earlier[0] * later[0], later[0] * earlier[1] + later[1])


def causal_taps(branch, filter_taps_weight):
    tap_count = filter_taps_weight.shape[0]
    positions = branch.shape[0]
    padded = jnp.pad(branch.astype(jnp.float32), ((tap_count - 1, 0), (0, 0)))
    running = jnp.zeros(branch.shape, jnp.float32)
    for offset in range(tap_count):
        running = running + padded[offset : offset + positions] * filter_taps_weight[offset].astype(
            jnp.float32
        )
    return running.astype(jnp.bfloat16)


def block_map(convolved, blocks):
    positions, channels = convolved.shape
    grouped = convolved.reshape(positions, blocks.shape[0], blocks.shape[1])
    mapped = jnp.einsum("sgi,gij->sgj", grouped, blocks, preferred_element_type=jnp.float32)
    return jax.nn.sigmoid(mapped.reshape(positions, channels))


def contract_columns(left, right):
    return lax.dot_general(
        left, right, (((1,), (1,)), ((), ())), preferred_element_type=jnp.float32
    )


def local(
    tokens,
    first_norm_scale,
    recurrent_branch_matrix,
    gelu_gate_matrix,
    filter_taps_weight,
    recurrence_gate_blocks,
    input_gate_blocks,
    base_decay_logits,
    extra_log_decay,
    mixer_output_matrix,
    second_norm_scale,
    mixer_up_matrix,
    mixer_down_matrix,
):
    positions = tokens.shape[0]
    own_count = positions // lax.axis_size("tp")
    normed = rms_scaled(tokens, first_norm_scale)
    branch_sum = jnp.dot(
        normed,
        lax.all_gather(recurrent_branch_matrix, "fs", axis=0, tiled=True),
        preferred_element_type=jnp.float32,
    )
    gate_sum = jnp.dot(
        normed,
        lax.all_gather(gelu_gate_matrix, "fs", axis=0, tiled=True),
        preferred_element_type=jnp.float32,
    )
    branch = branch_sum.astype(jnp.bfloat16)
    gate_branch = gate_sum.astype(jnp.bfloat16)
    out_full = lax.all_gather(mixer_output_matrix, "fs", axis=0, tiled=True)
    convolved = causal_taps(branch, filter_taps_weight)
    recurrence_gate_value = block_map(convolved, recurrence_gate_blocks)
    admission = block_map(convolved, input_gate_blocks)
    log_keep_factor = (
        decay_rate_scale * recurrence_gate_value * jax.nn.log_sigmoid(base_decay_logits)
        + extra_log_decay
    )
    retain = jnp.exp(log_keep_factor)
    driven = jnp.sqrt(-jnp.expm1(2.0 * log_keep_factor)) * (
        admission * convolved.astype(jnp.float32)
    )
    memory = lax.associative_scan(linear_combine, (retain, driven), axis=0)[1]
    recurrent = (memory * jax.nn.gelu(gate_branch.astype(jnp.float32))).astype(jnp.bfloat16)
    up_full = lax.all_gather(mixer_up_matrix, "fs", axis=0, tiled=True)
    whole_sum = lax.psum(contract_columns(recurrent, out_full).astype(jnp.bfloat16), "tp").astype(
        jnp.float32
    )
    residual_all = (tokens.astype(jnp.float32) + whole_sum).astype(jnp.bfloat16)
    raised = jnp.dot(
        rms_scaled(residual_all, second_norm_scale), up_full, preferred_element_type=jnp.float32
    )
    hidden = jnp.square(jax.nn.relu(raised)).astype(jnp.bfloat16)
    residual = lax.dynamic_slice_in_dim(
        residual_all, lax.axis_index("tp") * own_count, own_count, 0
    )
    down_full = lax.all_gather(mixer_down_matrix, "fs", axis=0, tiled=True)
    channel_sum = lax.psum_scatter(
        contract_columns(hidden, down_full).astype(jnp.bfloat16),
        "tp",
        scatter_dimension=0,
        tiled=True,
    ).astype(jnp.float32)
    return (residual.astype(jnp.float32) + channel_sum).astype(jnp.bfloat16)


MESH = pl.DeviceIdType.MESH
Y_SIZE = 2
MIX_GROUPS = 4
DOWN_GROUPS = 8
STEPPED = (0, 2)
X_FIRST = (0, 2)


def fits(mesh):
    n_fs, n_tp = mesh.shape["fs"], mesh.shape["tp"]
    return n_tp == 2 * Y_SIZE and n_fs == 4 * Y_SIZE


def shifted_down(values, by, fill):
    if by % 8 == 0:
        top = jnp.full((by, values.shape[1]), fill, values.dtype)
        return jnp.concatenate([top, values[: values.shape[0] - by]], axis=0)
    rows = lax.broadcasted_iota(jnp.int32, values.shape, 0)
    return jnp.where(rows < by, fill, pltpu.roll(values, by, 0))


def one_minus_exp(exponent):
    series = 1.0
    for order in range(8, 1, -1):
        series = 1.0 + exponent * (1.0 / order) * series
    return jnp.where(exponent > -0.35, -exponent * series, 1.0 - jnp.exp(exponent))


def fused(
    nz,
    tok_in, scale1_in, wb, wg, taps_in, rblk_in, iblk_in, logits_in, extra_in, wo, scale2_in, wu, wd,
    result,
    scale1, taps, rblk, iblk, logits, scale2,
    normed, fb, fg, fo, fu, fd, rdiag, idiag, tok, extra,
    part1, pair1, give1, got1, res, mid, hidden,
    part2, pair2, give2, got2, tally,
    s_sem, along, lump, across, r_recv, a_recv, b_recv, l_sem,
):
    f = lax.axis_index("fs")
    t = lax.axis_index("tp")
    z, y = f // Y_SIZE, f % Y_SIZE
    x, c = t // 2, t % 2
    last = nz - 1
    parity = z % 2
    at_end = (z == 0) | (z == last)
    zmate = z + 1 - 2 * parity
    ymate = z * Y_SIZE + (1 - y)
    xmate = (1 - x) * 2 + c
    cmate = x * 2 + (1 - c)
    diagonal = (1 - x) * 2 + (1 - c)
    rows, width = tok.shape
    own_rows = result.shape[0]
    depth = wb.shape[0]
    half = depth // 2
    units = fu.shape[1]

    barrier = pltpu.get_barrier_semaphore()

    def greet(sem, device):
        pl.semaphore_signal(sem, inc=1, device_id=device, device_id_type=MESH)

    to_x = {"fs": f, "tp": xmate}
    to_c = {"fs": f, "tp": cmate}
    to_z = {"fs": zmate * Y_SIZE + y, "tp": t}
    to_d = {"fs": zmate * Y_SIZE + y, "tp": xmate}
    inside = jnp.logical_not(at_end)
    for k in range(1, nz):
        greet(barrier, {"fs": lax.rem(z + k, nz) * Y_SIZE + y, "tp": t})
    for device in ({"fs": ymate, "tp": t}, to_x, to_c, to_d):
        greet(barrier, device)
    early = [
        pltpu.make_async_copy(given, kept, l_sem.at[1 + i])
        for i, (given, kept) in enumerate(
            (
                (tok_in, tok),
                (scale1_in, scale1),
                (rblk_in, rblk),
                (iblk_in, iblk),
                (taps_in, taps),
                (logits_in, logits),
                (extra_in, extra),
                (scale2_in, scale2),
            )
        )
    ]

    for copy in early:
        copy.start()
    pl.semaphore_wait(barrier, nz + 3)

    def start(pred, copy):
        if pred is None:
            copy.start()
        else:
            pl.when(pred)(copy.start)

    def settle(count, sem):
        lot = tally.at[pl.ds(0, count * 16), :]
        pltpu.make_async_copy(lot, lot, sem).wait()

    plain = (wb, wg, wo)
    whole = (fb, fg, fo)
    lumped, single = (0, 1, 3, 4), (2, 5, 6)

    def source(g, way_parity):
        if g < 3:
            return plain[g]
        w = wu if g < 5 else wd
        first = half * ((g - 3) % 2)
        return w.at[
            pl.ds(first, half), pl.ds(pl.multiple_of(way_parity * units, units), units)
        ]

    def slot(g, zs, ys):
        if g < 3:
            return whole[g].at[pl.ds(pl.multiple_of((zs * Y_SIZE + ys) * depth, depth), depth), :]
        if g < 5:
            at = (zs * Y_SIZE + ys) * depth + (g - 3) * half
            return fu.at[pl.ds(pl.multiple_of(at, half), half), :]
        at = ((zs * 2 + (g - 5)) * Y_SIZE + ys) * half
        return fd.at[pl.ds(pl.multiple_of(at, half), half), :]

    def over(g, zs):
        return lump.at[lumped.index(g)] if g in lumped else across.at[single.index(g), zs]

    def z_copy(g, src, zs, zt):
        return pltpu.make_async_remote_copy(
            src_ref=src,
            dst_ref=slot(g, zs, y),
            send_sem=s_sem.at[0 if g < 3 else 1],
            recv_sem=along.at[g, zs],
            device_id={"fs": zt * Y_SIZE + y, "tp": t},
            device_id_type=MESH,
        )

    def y_copy(g, src, zs):
        return pltpu.make_async_remote_copy(
            src_ref=src,
            dst_ref=slot(g, zs, y),
            send_sem=s_sem.at[2],
            recv_sem=over(g, zs),
            device_id={"fs": ymate, "tp": t},
            device_id_type=MESH,
        )

    def landed(here, sem):
        pltpu.make_async_copy(here, here, sem).wait()

    def take(g, zs):
        landed(slot(g, zs, y), along.at[g, zs])

    def spread_z(g, outer=None, far=range(1, nz), held=None):
        for d in (1,) if g < 3 else far:
            for way in (0, 1):
                zt = z + d if way == 0 else z - d
                exists = zt <= last if way == 0 else zt >= 0
                if outer is not None:
                    to_end = (zt == 0) | (zt == last)
                    exists = exists & (to_end if outer else jnp.logical_not(to_end))
                if held is not None:
                    exists = exists & (at_end if held else jnp.logical_not(at_end))
                start(exists, z_copy(g, source(g, lax.rem(zt + nz, 2)), z, zt))

    def own(g, pred=None):
        start(pred, y_copy(g, source(g, parity), z))

    def forward(g, d):
        for way in (0, 1):
            zs = z - d if way == 0 else z + d
            exists = zs >= 0 if way == 0 else zs <= last
            pl.when(exists)(functools.partial(take, g, zs))
            if d < last:
                onward = z < last if way == 0 else z > 0
                zt = z + 1 if way == 0 else z - 1
                start(exists & onward, z_copy(g, slot(g, zs, y), zs, zt))
            start(exists, y_copy(g, slot(g, zs, y), zs))

    side = z // (nz // 2)
    origins = [zmate] + [rank + side * (last - 2 * rank) for rank in range(2, nz)]

    def hand_over(g, k, pred=None):
        if pred is None:
            take(g, origins[k])
        else:
            pl.when(pred)(functools.partial(take, g, origins[k]))
        start(pred, y_copy(g, slot(g, origins[k], y), origins[k]))

    def take_lump(g):
        count = nz * depth if g < 3 else nz * half
        landed((whole[g] if g < 3 else fu).at[pl.ds(0, count), :], over(g, 0))

    def take_over(g, zs):
        landed(slot(g, zs, 1 - y), over(g, zs))

    def near_copy(src, dst, device, sem):
        copy = pltpu.make_async_remote_copy(
            src_ref=src,
            dst_ref=dst,
            send_sem=s_sem.at[3],
            recv_sem=sem,
            device_id=device,
            device_id_type=MESH,
        )
        copy.start()
        return copy

    spread_z(0)
    own(0)
    spread_z(1)
    own(1)

    stays = [
        pltpu.make_async_copy(source(g, parity), slot(g, z, y), l_sem.at[0]) for g in range(7)
    ]
    for copy in stays:
        copy.start()
    for copy in early:
        copy.wait()
    block = rblk.shape[1]
    for blocks, diag in ((rblk, rdiag), (iblk, idiag)):
        diag[...] = jnp.zeros_like(diag)
        for b in range(rblk.shape[0]):
            diag[b * block : (b + 1) * block, b * block : (b + 1) * block] = blocks[b]

    def norm_rows(i, carry):
        at = pl.ds(pl.multiple_of(i * 32, 32), 32)
        normed[at, :] = rms_scaled(tok[at, :], scale1[...])
        return carry

    lax.fori_loop(0, rows // 32, norm_rows, 0)

    forward(0, 1)
    forward(1, 1)
    forward(0, 2)
    own(2)
    forward(1, 2)
    spread_z(2)
    forward(0, 3)
    forward(1, 3)
    forward(2, 1)
    spread_z(3, False)
    spread_z(4, False)
    settle(depth // 16 * 7, l_sem.at[0])
    take_lump(0)

    branch = jnp.dot(normed[...], fb[...], preferred_element_type=jnp.float32)
    branch = branch.astype(jnp.bfloat16).astype(jnp.float32)
    tap_count = taps.shape[0]
    running = branch * taps[tap_count - 1 : tap_count, :].astype(jnp.float32)
    for offset in range(tap_count - 1):
        by = tap_count - 1 - offset
        running = running + shifted_down(branch, by, 0.0) * taps[offset : offset + 1, :].astype(
            jnp.float32
        )
    convolved = running.astype(jnp.bfloat16)
    rate = jax.nn.sigmoid(jnp.dot(convolved, rdiag[...], preferred_element_type=jnp.float32))
    admission = jax.nn.sigmoid(jnp.dot(convolved, idiag[...], preferred_element_type=jnp.float32))
    base = -jnp.log1p(jnp.exp(-logits[...]))
    log_keep = decay_rate_scale * rate * base + extra[...]
    keep = jnp.exp(log_keep)
    memory = jnp.sqrt(one_minus_exp(2.0 * log_keep)) * (admission * convolved.astype(jnp.float32))
    by = 1
    while by < rows:
        memory = keep * shifted_down(memory, by, 0.0) + memory
        if 2 * by < rows:
            keep = keep * shifted_down(keep, by, 1.0)
        by *= 2
    forward(2, 2)
    take_lump(1)
    gate = jnp.dot(normed[...], fg[...], preferred_element_type=jnp.float32)
    gate = gate.astype(jnp.bfloat16).astype(jnp.float32)
    recurrent = (memory * jax.nn.gelu(gate)).astype(jnp.bfloat16)

    forward(2, 3)
    spread_z(3, True)
    spread_z(4, True)
    spread_z(5, False, held=False)
    spread_z(6, False, held=False)
    own(3)
    own(4)
    own(5, at_end)
    hand_over(3, 1, inside)
    hand_over(4, 1, inside)
    own(5, inside)

    inner = z + side * (last - 2 * z)
    ranks = [inner, 1 - inner] + list(range(2, nz))
    order = [rank + side * (last - 2 * rank) for rank in ranks]
    span = width // MIX_GROUPS
    own_at = pl.ds(pl.multiple_of(t * own_rows, own_rows), own_rows)
    firsts, seconds = [], []

    def mix_columns(j):
        return pl.ds(pl.multiple_of(order[j] * span, span), span)

    def mix_first(j):
        firsts[j].wait_recv()
        away = part1[j, 1 - x, c].astype(jnp.float32) + pair1[j, 1 - x].astype(jnp.float32)
        give1[j] = away.astype(jnp.bfloat16)
        seconds.append(
            near_copy(give1.at[j], got1.at[j], to_x, r_recv.at[MIX_GROUPS + j])
        )

    def mix_second(j):
        seconds[j].wait_recv()
        mixed = part1[j, x, c].astype(jnp.float32) + pair1[j, x].astype(jnp.float32)
        mixed = mixed + got1[j].astype(jnp.float32)
        at = mix_columns(j)
        res[:, at] = (tok[own_at, at].astype(jnp.float32) + mixed).astype(jnp.bfloat16)

    for j in range(MIX_GROUPS):
        if j == 2:
            mix_first(1)
        take_over(2, order[j])
        product = contract_columns(recurrent, fo[mix_columns(j), :])
        part1[j] = product.astype(jnp.bfloat16).reshape(2, 2, own_rows, span)
        firsts.append(
            near_copy(part1.at[j, :, 1 - c], pair1.at[j], to_c, r_recv.at[j])
        )
        if j == 1:
            mix_first(0)
        if j > 1:
            mix_first(j)
    for j in range(MIX_GROUPS):
        mix_second(j)

    mid[parity, t] = rms_scaled(res[...], scale2[...])
    mine = mid.at[parity, t]
    theirs = mid.at[1 - parity, t]
    near_copy(mine, mine, to_x, a_recv.at[1])
    near_copy(mine, mine, to_z, a_recv.at[0])
    near_copy(mine, mine, to_c, a_recv.at[2])
    spread_z(5, False, held=True)
    spread_z(6, False, held=True)
    spread_z(5, True, (1,))
    spread_z(6, True, (1,))

    def arrived(here, index):
        landed(here, a_recv.at[index])

    def pass_on(here, device, index):
        near_copy(here, here, device, a_recv.at[index])

    beside = mid.at[parity, xmate]
    askew = mid.at[1 - parity, xmate]
    for g in (3, 4):
        for k in range(nz - 1):
            hand_over(g, k, at_end if k == 1 else None)
    own(6)
    arrived(beside, 1)
    pass_on(beside, to_c, 5)
    arrived(theirs, 0)
    pass_on(theirs, to_x, 3)
    pass_on(theirs, to_c, 4)
    spread_z(5, True, range(2, nz))
    spread_z(6, True, range(2, nz))
    arrived(mid.at[parity, cmate], 2)
    arrived(mid.at[parity, diagonal], 5)
    take_lump(3)
    take_lump(4)

    tile = 256

    def up(par):
        def up_tile(i, carry):
            at = pl.ds(pl.multiple_of(i * tile, tile), tile)
            raised = jnp.dot(
                mid[par].reshape(rows, width), fu[:, at], preferred_element_type=jnp.float32
            )
            hidden[par, :, at] = jnp.square(jnp.maximum(raised, 0.0)).astype(jnp.bfloat16)
            return carry

        lax.fori_loop(0, units // tile, up_tile, 0)

    up(parity)
    hand_over(5, 0)
    arrived(askew, 3)
    pass_on(askew, to_c, 6)
    arrived(mid.at[1 - parity, cmate], 4)
    arrived(mid.at[1 - parity, diagonal], 6)
    up(1 - parity)

    narrow = width // DOWN_GROUPS
    halves = [k for r in range(2) for k in range(2)] + [k for k in range(2) for r in range(2, nz)]
    final = DOWN_GROUPS - 1
    lots = [(j, None) for j in range(final - 1)] + [(final, 0), (final - 1, None), (final, 1)]
    shared, spread = {}, {}
    level = jnp.where(at_end, 0, 1)

    def number(lot):
        j, which = lot
        if j >= 4:
            return j + (which or 0)
        return (level if j < 2 else 1 - level) * 2 + j % 2

    def place(j):
        if j < 4:
            return z if j < 2 else zmate
        rank = 2 + (j - 4) % (nz - 2)
        return rank + side * (last - 2 * rank)

    def signal_at(lot, k):
        return b_recv.at[number(lot), k]

    def lot_columns(lot):
        which = lot[1]
        return pl.ds(0, narrow if which is None else half)

    def lot_sides(lot):
        which = lot[1]
        return list(range(Y_SIZE)) if which is None else [y if which == 0 else 1 - y]

    def pair_sum(lot, par, xs):
        at = lot_columns(lot)
        mine = part2[number(lot), par, xs, c, :, at].astype(jnp.float32)
        return mine + pair2[number(lot), par, xs, :, at].astype(jnp.float32)

    def multiply(i):
        lot = lots[i]
        j, which = lot
        q = place(j)
        if which != 0:
            take_over(5 + halves[j], q)
        first = (q * 2 + halves[j]) * narrow
        if which is not None:
            first = first + lot_sides(lot)[0] * half
        at = lot_columns(lot)
        some = fd[pl.ds(pl.multiple_of(first, half), at.size), :]
        product = contract_columns(hidden[...].reshape(2 * rows, units), some)
        n = number(lot)
        part2[n, :, :, :, :, at] = product.astype(jnp.bfloat16).reshape(2, 2, 2, own_rows, at.size)
        shared[lot] = near_copy(
            part2.at[n, :, :, 1 - c, :, at], pair2.at[n, :, :, :, at], to_c, signal_at(lot, 0)
        )

    def exchange(i):
        lot = lots[i]
        shared[lot].wait_recv()
        at = lot_columns(lot)
        n = number(lot)
        if i in STEPPED:
            for k in range(2):
                away = pair_sum(lot, k, 1 - x) if i in X_FIRST else pair_sum(lot, 1 - parity, k)
                give2[n, k] = away.astype(jnp.bfloat16)
            two = pl.ds(0, 2)
            device = to_x if i in X_FIRST else to_z
            spread[lot] = [
                near_copy(give2.at[n, two], got2.at[n, two], device, signal_at(lot, 1))
            ]
            return
        ways = [
            (to_d, 1 - parity, 1 - x),
            (to_x, parity, 1 - x),
            (to_z, 1 - parity, x),
        ]
        spread[lot] = []
        for k, (device, par, xs) in enumerate(ways):
            give2[n, k, :, at] = pair_sum(lot, par, xs).astype(jnp.bfloat16)
            spread[lot].append(
                near_copy(
                    give2.at[n, k, :, at], got2.at[n, k, :, at], device, signal_at(lot, 1)
                )
            )

    def pass_across(i):
        lot = lots[i]
        spread[lot][0].wait_recv()
        n = number(lot)
        if i in X_FIRST:
            away = pair_sum(lot, 1 - parity, x) + got2[n, 1 - parity].astype(jnp.float32)
        else:
            away = pair_sum(lot, parity, 1 - x) + got2[n, 1 - x].astype(jnp.float32)
        give2[n, 2] = away.astype(jnp.bfloat16)
        device = to_z if i in X_FIRST else to_x
        spread[lot] = [near_copy(give2.at[n, 2], got2.at[n, 2], device, signal_at(lot, 2))]

    def finish(i):
        lot = lots[i]
        if i in STEPPED:
            spread[lot][0].wait_recv()
        else:
            landed(got2.at[number(lot), :, :, lot_columns(lot)], signal_at(lot, 1))
        total = pair_sum(lot, parity, x)
        for k in [parity if i in X_FIRST else x, 2] if i in STEPPED else range(3):
            total = total + got2[number(lot), k, :, lot_columns(lot)].astype(jnp.float32)
        for k, ys in enumerate(lot_sides(lot)):
            first = (place(lot[0]) * Y_SIZE + ys) * depth + halves[lot[0]] * half
            at = pl.ds(pl.multiple_of(first, half), half)
            result[:, at] = (
                res[:, at].astype(jnp.float32) + total[:, k * half : (k + 1) * half]
            ).astype(jnp.bfloat16)

    plan = [
        (hand_over, 6, 0),
        (multiply, 0),
        (multiply, 1),
        (exchange, 0),
        (exchange, 1),
        (multiply, 2),
        (hand_over, 5, 1),
        (exchange, 2),
        (hand_over, 5, 2),
        (multiply, 3),
        (exchange, 3),
        (hand_over, 6, 1),
        (multiply, 4),
        (pass_across, 0),
        (exchange, 4),
        (hand_over, 6, 2),
        (multiply, 5),
        (exchange, 5),
        (pass_across, 2),
        (multiply, 6),
        (exchange, 6),
        (multiply, 7),
        (exchange, 7),
        (multiply, 8),
        (exchange, 8),
        (finish, 4),
        (finish, 5),
        (finish, 6),
        (finish, 0),
        (finish, 1),
        (finish, 2),
        (finish, 3),
        (finish, 7),
        (finish, 8),
    ]
    for step, *which in plan:
        step(*which)
    pl.when(at_end)(functools.partial(settle, depth // 16 * 3, s_sem.at[0]))
    relayed = 3 * (2 + nz - 1)
    pl.when(inside)(functools.partial(settle, depth // 16 * relayed, s_sem.at[0]))
    settle(depth // 16 * 4 * (nz - 1), s_sem.at[1])
    settle(depth // 16 * 7 * nz, s_sem.at[2])
    bits = own_rows * width // (16 * depth)
    mixed = own_rows * span // (16 * depth)
    summed = own_rows * narrow // (16 * depth)
    settle(7 * bits + 3 * MIX_GROUPS * mixed + 7 * DOWN_GROUPS * summed, s_sem.at[3])


def fused_local(
    mesh,
    tokens,
    first_norm_scale,
    recurrent_branch_matrix,
    gelu_gate_matrix,
    filter_taps_weight,
    recurrence_gate_blocks,
    input_gate_blocks,
    base_decay_logits,
    extra_log_decay,
    mixer_output_matrix,
    second_norm_scale,
    mixer_up_matrix,
    mixer_down_matrix,
):
    n_fs, n_tp = mesh.shape["fs"], mesh.shape["tp"]
    rows, width = tokens.shape
    own_rows = rows // n_tp
    channels = recurrent_branch_matrix.shape[1]
    units = mixer_up_matrix.shape[1] // 2
    span = width // MIX_GROUPS
    narrow = width // DOWN_GROUPS
    low, high = jnp.bfloat16, jnp.float32
    hbm = pl.BlockSpec(memory_space=pl.ANY)
    return pl.pallas_call(
        functools.partial(fused, n_fs // Y_SIZE),
        out_shape=pltpu.VMEM((own_rows, width), low),
        in_specs=[hbm] * 13,
        out_specs=pl.BlockSpec(memory_space=pltpu.VMEM),
        scratch_shapes=[
            pltpu.VMEM((1, width), high),
            pltpu.VMEM(filter_taps_weight.shape, low),
            pltpu.VMEM(recurrence_gate_blocks.shape, low),
            pltpu.VMEM(input_gate_blocks.shape, low),
            pltpu.VMEM((1, channels), high),
            pltpu.VMEM((1, width), high),
            pltpu.VMEM((rows, width), low),
            pltpu.VMEM((width, channels), low),
            pltpu.VMEM((width, channels), low),
            pltpu.VMEM((width, channels), low),
            pltpu.VMEM((width, units), low),
            pltpu.VMEM((width, units), low),
            pltpu.VMEM((channels, channels), low),
            pltpu.VMEM((channels, channels), low),
            pltpu.VMEM((rows, width), low),
            pltpu.VMEM((rows, channels), high),
            pltpu.VMEM((MIX_GROUPS, 2, 2, own_rows, span), low),
            pltpu.VMEM((MIX_GROUPS, 2, own_rows, span), low),
            pltpu.VMEM((MIX_GROUPS, own_rows, span), low),
            pltpu.VMEM((MIX_GROUPS, own_rows, span), low),
            pltpu.VMEM((own_rows, width), low),
            pltpu.VMEM((2, n_tp, own_rows, width), low),
            pltpu.VMEM((2, rows, units), low),
            pltpu.VMEM((DOWN_GROUPS + 1, 2, 2, 2, own_rows, narrow), low),
            pltpu.VMEM((DOWN_GROUPS + 1, 2, 2, own_rows, narrow), low),
            pltpu.VMEM((DOWN_GROUPS + 1, 3, own_rows, narrow), low),
            pltpu.VMEM((DOWN_GROUPS + 1, 3, own_rows, narrow), low),
            pltpu.VMEM((16 * 1024, width // 8), low),
            pltpu.SemaphoreType.DMA((4,)),
            pltpu.SemaphoreType.DMA((7, n_fs // Y_SIZE)),
            pltpu.SemaphoreType.DMA((4,)),
            pltpu.SemaphoreType.DMA((3, n_fs // Y_SIZE)),
            pltpu.SemaphoreType.DMA((2 * MIX_GROUPS,)),
            pltpu.SemaphoreType.DMA((7,)),
            pltpu.SemaphoreType.DMA((DOWN_GROUPS + 1, 3)),
            pltpu.SemaphoreType.DMA((9,)),
        ],
        compiler_params=pltpu.CompilerParams(
            collective_id=0, has_side_effects=True, vmem_limit_bytes=60 * 1024 * 1024
        ),
        name="fused_layer",
    )(
        tokens,
        first_norm_scale.reshape(1, width),
        recurrent_branch_matrix,
        gelu_gate_matrix,
        filter_taps_weight,
        recurrence_gate_blocks,
        input_gate_blocks,
        base_decay_logits.reshape(1, channels),
        extra_log_decay,
        mixer_output_matrix,
        second_norm_scale.reshape(1, width),
        mixer_up_matrix,
        mixer_down_matrix,
    )


def solution(mesh):
    in_specs = (
        P("fs", None),
        P(),
        P("fs", "tp"),
        P("fs", "tp"),
        P(None, "tp"),
        P("tp", None, None),
        P("tp", None, None),
        P("tp"),
        P("fs", "tp"),
        P("fs", "tp"),
        P(),
        P("fs", "tp"),
        P("fs", "tp"),
    )
    out_specs = P(("fs", "tp"), None)
    body = functools.partial(fused_local, mesh) if fits(mesh) else local
    return jax.shard_map(body, mesh=mesh, in_specs=in_specs, out_specs=out_specs, check_vma=False)
```
